32 devices in a mesh: dp: 4 (over y, x), kv: 4 (over z), tp: 2 (over core).
Axes of the slice: x: 2, y: 2, z: 4, core: 2. Of those that a mesh axis runs over, the one named last changes fastest.
Arguments:
- tokens: bfloat16 [32, 4096], P('dp', ('kv', 'tp')), may hold values from -27 to 27
- lengths: int32 [32], P(('dp', 'kv')), may hold values from 1 to 64, 512 in all
- state: float32 [32, 4, 384, 768], P(('dp', 'kv'), 'tp'), may hold values from -6 to 6
- cache_keys: bfloat16 [32, 4, 64, 384], P(('dp', 'kv'), 'tp'), may hold values from -6 to 6
- cache_values: bfloat16 [32, 4, 64, 768], P(('dp', 'kv'), 'tp'), may hold values from -6 to 6
- cache_rates: float32 [32, 4, 64, 384], P(('dp', 'kv'), 'tp'), may hold values from 0.002 to 0.3
- attn_gain: bfloat16 [4096], P('kv'), may hold values from 0.099609375 to 1.8984375
- w_query: bfloat16 [4096, 1536], P('kv', 'tp'), may hold values from -0.09375 to 0.09375
- w_key: bfloat16 [4096, 1536], P('kv', 'tp'), may hold values from -0.09375 to 0.09375
- w_value: bfloat16 [4096, 3072], P('kv', 'tp'), may hold values from -0.09375 to 0.09375
- w_gate: bfloat16 [4096, 3072], P('kv', 'tp'), may hold values from -0.09375 to 0.09375
- w_decay: bfloat16 [4096, 1536], P('kv', 'tp'), may hold values from -0.375 to 0.375
- head_gain: bfloat16 [4, 768], P('tp'), may hold values from 0.099609375 to 1.8984375
- w_out: bfloat16 [3072, 4096], P(None, ('kv', 'tp')), may hold values from -0.109375 to 0.109375
- mlp_gain: bfloat16 [4096], replicated, may hold values from 0.099609375 to 1.8984375
- w_mlp_gate: bfloat16 [4096, 11008], P(None, ('kv', 'tp')), may hold values from -0.09375 to 0.09375
- w_mlp_up: bfloat16 [4096, 11008], P(None, ('kv', 'tp')), may hold values from -0.09375 to 0.09375
- w_mlp_down: bfloat16 [11008, 4096], P(('kv', 'tp')), may hold values from -0.078125 to 0.078125
Outputs:
- result: bfloat16 [32, 4096], P('dp', ('kv', 'tp'))
The draws below stay inside these ranges and needn't reach their ends.
Inputs may be any that keep to these rules, and one draw needn't show every extreme that they name: `lengths`: each sequence's count of live slots in its block cache; slots from that count on take no part.
All inputs are finite; a program needn't handle non-finite values.
Results may differ from the reference program's by a relative error of at most 0.0085.
Values may be sent and summed in bfloat16 or wider, within the bound.
No kernel may reach another device: no remote copies, remote signals or barrier semaphores. Data moves between devices by JAX's collectives and lax.ppermute only.
A program may use at most 128 MiB of HBM per device.

```python
import math
import jax
import jax.numpy as jnp
import numpy as np
from jax import lax

D = 4096
HEADS = 4
DK = 384
DV = 768
FF = 11008
SPAN = 64
SEQS = 32


def draw_tokens(key, part):
    base_key = jax.random.fold_in(key, 11)
    rough_key = jax.random.fold_in(key, 12)
    columns = jnp.arange(D, dtype=jnp.float32)
    rising = jnp.exp(jnp.log(3.0) * columns / (D - 1))
    rough = jax.random.uniform(rough_key, (D,), jnp.float32, 0.5, 1.5)
    values = jnp.clip(jax.random.normal(base_key, (SEQS, D), jnp.float32), -6.0, 6.0)
    return (values * rising[None, :] * rough[None, :]).astype(jnp.bfloat16)


def raised(values, stream_key, source, target, shards_of, factor):
    owner, partner = [(jnp.arange(values.shape[position]) // (values.shape[position] // shards_of)).reshape([-1 if axis == position else 1 for axis in range(values.ndim)]) for position in (source, target)]
    chosen = jax.random.permutation(stream_key, shards_of)[partner]
    strong = (owner == chosen) | (owner == (partner + shards_of // 2) % shards_of)
    return jnp.where(strong, factor * values, values)


def levels(key, extent, pieces, low, high):
    gain = 1.0
    for axis_at, shards_of in pieces:
        draws = jax.random.uniform(jax.random.fold_in(jax.random.fold_in(key, 6), axis_at), (shards_of,), jnp.float32, low / len(pieces), high / len(pieces))
        gain = gain * jnp.repeat(jnp.exp(draws), extent[axis_at] // shards_of).reshape((-1,) + (1,) * (len(extent) - 1 - axis_at))
    return gain


def split_up(amount, total, reach, skew):
    loads = [(1 << 20) // math.isqrt(grade ** skew) + 1 for grade in range(2, amount + 1)]
    surplus, holding = total - reach - (amount - 1), [1] * (amount - 1)
    while surplus > 0:
        candidates = [i for i in range(amount - 1) if holding[i] < reach]
        pool, remaining = sum([loads[i] for i in candidates]), surplus
        for i in candidates:
            extra = min(reach - holding[i], max(1, remaining * loads[i] // pool), surplus)
            holding[i] = holding[i] + extra
            surplus = surplus - extra
    return np.array([reach] + holding)


def ragged(stream_key, count, total, bound, lean):
    if count == 2:
        one = jax.random.randint(stream_key, (), max(1, total - bound), min(bound, total - 1) + 1)
        return jnp.stack([one, total - one])
    sizes = jnp.asarray(split_up(count, total, bound, lean), jnp.int32)
    pairs = (count - 1) // 2
    giver, taker = sizes[1:1 + 2 * pairs:2], sizes[2:2 + 2 * pairs:2]
    margin = jnp.minimum(giver - 1, bound - taker)
    shifted = jax.random.randint(jax.random.fold_in(stream_key, 1), (pairs,), 0, 1 << 20) % (margin + 1)
    sizes = sizes.at[1:1 + 2 * pairs:2].set(giver - shifted).at[2:2 + 2 * pairs:2].set(taker + shifted)
    return sizes[jax.random.permutation(jax.random.fold_in(stream_key, 2), count)]


def gaussian(stream_key, extent, spread, most, split=(), held_as=jnp.bfloat16):
    factor_of = levels(stream_key, extent, split, -0.22, 0.18) if split else 1.0
    entries = jax.random.normal(stream_key, extent, jnp.float32) * spread * factor_of
    return jnp.minimum(jnp.maximum(entries, -most), most).astype(held_as)


def bell_draw_with(own_key, extent, width, bound, shards, heavy, kind=jnp.bfloat16):
    drawn = width * jax.random.normal(own_key, extent, jnp.float32)
    if shards:
        drawn = drawn * levels(own_key, extent, shards, -0.22, 0.18)
    return jnp.clip(raised(drawn, jax.random.fold_in(own_key, 3), *heavy), -bound, bound).astype(kind)


def setup_inputs(seed: int = 0) -> dict:
    streams_of = jax.random.split(jax.random.key(seed), 19)
    tokens = draw_tokens(jax.random.fold_in(streams_of[18], 71), 0)
    lengths = ragged(streams_of[1], SEQS, SEQS * SPAN // 4, SPAN, 2).astype(jnp.int32)
    state = gaussian(streams_of[2], (SEQS, HEADS, DK, DV), 1.0, 6.0, ((0, 16), (1, 2)), jnp.float32)
    cache_keys = gaussian(streams_of[3], (SEQS, HEADS, SPAN, DK), 1.0, 6.0, ((0, 16), (1, 2)))
    cache_values = gaussian(streams_of[4], (SEQS, HEADS, SPAN, DV), 1.0, 6.0, ((0, 16), (1, 2)))
    cache_rates = jnp.clip(jnp.exp(math.log(0.3) - 5.0106353 * jax.random.uniform(streams_of[5], (SEQS, HEADS, SPAN, DK), jnp.float32) ** levels(streams_of[5], (SEQS, HEADS, SPAN, DK), ((0, 16), (1, 2)), -0.2, 0.2)), 0.002, 0.3)
    attn_gain = jnp.clip(1.0 + 0.18 * jax.random.normal(streams_of[6], (D,), jnp.float32), 0.099609375, 1.8984375).astype(jnp.bfloat16)
    w_query = gaussian(streams_of[7], (D, HEADS * DK), D ** -0.5, 0.09375, ((0, 4), (1, 2)))
    w_key = gaussian(streams_of[8], (D, HEADS * DK), D ** -0.5, 0.09375, ((0, 4), (1, 2)))
    w_value = gaussian(streams_of[9], (D, HEADS * DV), D ** -0.5, 0.09375, ((0, 4), (1, 2)))
    w_gate = gaussian(streams_of[10], (D, HEADS * DV), D ** -0.5, 0.09375, ((0, 4), (1, 2)))
    w_decay = gaussian(streams_of[11], (D, HEADS * DK), (D // 16) ** -0.5, 0.375, ((0, 4), (1, 2)))
    head_gain = jnp.clip(1.0 + 0.18 * jax.random.normal(streams_of[12], (HEADS, DV), jnp.float32), 0.099609375, 1.8984375).astype(jnp.bfloat16)
    w_out = gaussian(streams_of[13], (HEADS * DV, D), (HEADS * DV) ** -0.5, 0.109375, ((1, 8),))
    mlp_gain = jnp.clip(1.0 + 0.18 * jax.random.normal(streams_of[14], (D,), jnp.float32), 0.099609375, 1.8984375).astype(jnp.bfloat16)
    w_mlp_gate = gaussian(streams_of[15], (D, FF), D ** -0.5, 0.09375, ((1, 8),))
    w_mlp_up = gaussian(streams_of[16], (D, FF), D ** -0.5, 0.09375, ((1, 8),))
    w_mlp_down = bell_draw_with(streams_of[17], (FF, D), FF ** -0.5, 0.078125, ((0, 8),), (0, 1, 8, 2.0))
    return dict(tokens=tokens, lengths=lengths, state=state, cache_keys=cache_keys, cache_values=cache_values, cache_rates=cache_rates, attn_gain=attn_gain, w_query=w_query, w_key=w_key, w_value=w_value, w_gate=w_gate, w_decay=w_decay, head_gain=head_gain, w_out=w_out, mlp_gain=mlp_gain, w_mlp_gate=w_mlp_gate, w_mlp_up=w_mlp_up, w_mlp_down=w_mlp_down)


EPS = 1e-06
GATE_NORM = 16.0
exact_mode = lax.Precision.HIGHEST

def front_part(query, key_new, log_decay, state, cache_keys, cache_rates, lengths):
    span = cache_keys.shape[2]
    live = (jnp.arange(span, dtype=jnp.int32)[None, :] < lengths[:, None]).astype(jnp.float32)
    running = jnp.cumsum(cache_rates * live[:, None, :, None], axis=2)
    total = running[:, :, -1:, :]
    weight = jnp.exp(running - total + log_decay[:, :, None, :])
    scores = jnp.einsum('bhd,bhjd->bhj', query, weight * cache_keys.astype(jnp.float32), precision=exact_mode) * live[:, None, :]
    carried = jnp.einsum('bhd,bhde->bhe', query * jnp.exp(log_decay - total[:, :, 0, :]), state, precision=exact_mode)
    own = lax.optimization_barrier(jnp.sum(query * key_new, axis=-1, keepdims=True))
    return (scores, carried, own)

def back_part(scores, carried, own, value_new, cache_values, gate, head_gain):
    inner = jnp.einsum('bhj,bhje->bhe', scores, cache_values.astype(jnp.float32), precision=exact_mode)
    attended = carried + inner + own * value_new
    normed = attended * lax.rsqrt(lax.optimization_barrier(jnp.mean(attended * attended, axis=-1, keepdims=True)) + EPS)
    normed = normed * head_gain.astype(jnp.float32)
    return (jax.nn.silu(gate) * normed).astype(jnp.bfloat16)

def reference(tokens, lengths, state, cache_keys, cache_values, cache_rates, attn_gain, w_query, w_key, w_value, w_gate, w_decay, head_gain, w_out, mlp_gain, w_mlp_gate, w_mlp_up, w_mlp_down):
    seqs = tokens.shape[0]
    heads_all, key_dim, value_dim = (state.shape[1], state.shape[2], state.shape[3])
    wide = tokens.astype(jnp.float32)
    inv_rms = lax.rsqrt(lax.optimization_barrier(jnp.mean(wide * wide, axis=1, keepdims=True)) + EPS)
    scaled = (wide * attn_gain.astype(jnp.float32)).astype(jnp.bfloat16)

    def project(matrix):
        return jnp.dot(scaled, matrix, preferred_element_type=jnp.float32) * inv_rms
    query = (project(w_query) * key_dim ** (-0.5)).reshape(seqs, heads_all, key_dim)
    key_new = project(w_key).reshape(seqs, heads_all, key_dim)
    log_decay = (jax.nn.log_sigmoid(project(w_decay)) / GATE_NORM).reshape(seqs, heads_all, key_dim)
    value_new = project(w_value).reshape(seqs, heads_all, value_dim)
    gate = project(w_gate).reshape(seqs, heads_all, value_dim)
    scores, carried, own = front_part(query, key_new, log_decay, state, cache_keys, cache_rates, lengths)
    heads = back_part(scores, carried, own, value_new, cache_values, gate, head_gain)
    heads = heads.reshape(seqs, heads_all * value_dim)
    after = (wide + jnp.dot(heads, w_out, preferred_element_type=jnp.float32)).astype(jnp.bfloat16)
    second = after.astype(jnp.float32)
    inv_second = lax.rsqrt(lax.optimization_barrier(jnp.mean(second * second, axis=1, keepdims=True)) + EPS)
    normed = (second * inv_second * mlp_gain.astype(jnp.float32)).astype(jnp.bfloat16)
    gate_ff = jnp.dot(normed, w_mlp_gate, preferred_element_type=jnp.float32)
    up_ff = jnp.dot(normed, w_mlp_up, preferred_element_type=jnp.float32)
    hidden = (jax.nn.silu(gate_ff) * up_ff).astype(jnp.bfloat16)
    return (second + jnp.dot(hidden, w_mlp_down, preferred_element_type=jnp.float32)).astype(jnp.bfloat16)
```

```python
import jax
import jax.numpy as jnp
from jax import lax
from jax.experimental import pallas as pl
from jax.experimental.pallas import tpu as pltpu
from jax.sharding import PartitionSpec as P

EPS = 1e-06
GATE_NORM = 16.0
exact_mode = lax.Precision.HIGHEST


def front_part(query, key_new, log_decay, state, cache_keys, cache_rates, lengths):
    span = cache_keys.shape[2]
    live = (jnp.arange(span, dtype=jnp.int32)[None, :] < lengths[:, None]).astype(jnp.float32)
    running = jnp.cumsum(cache_rates * live[:, None, :, None], axis=2)
    total = running[:, :, -1:, :]
    weight = jnp.exp(running - total + log_decay[:, :, None, :])
    scores = (
        jnp.einsum(
            "bhd,bhjd->bhj", query, weight * cache_keys.astype(jnp.float32), precision=exact_mode
        )
        * live[:, None, :]
    )
    carried = jnp.einsum(
        "bhd,bhde->bhe", query * jnp.exp(log_decay - total[:, :, 0, :]), state, precision=exact_mode
    )
    own = jnp.sum(query * key_new, axis=-1, keepdims=True)
    return (scores, carried, own)


def back_part(scores, carried, own, value_new, cache_values, gate, head_gain):
    inner = jnp.einsum(
        "bhj,bhje->bhe", scores, cache_values.astype(jnp.float32), precision=exact_mode
    )
    attended = carried + inner + own * value_new
    normed = attended * lax.rsqrt(jnp.mean(attended * attended, axis=-1, keepdims=True) + EPS)
    normed = normed * head_gain.astype(jnp.float32)
    return (jax.nn.silu(gate) * normed).astype(jnp.bfloat16)


def open_heads(
    query_sum, key_sum, decay_sum, own_squares, width, state, cache_keys, cache_rates, lengths
):
    seq_dev, heads_dev, key_dim = (state.shape[0], state.shape[1], state.shape[2])
    inv_rms = lax.rsqrt(own_squares / width + EPS)[:, None]
    query = (query_sum * inv_rms * key_dim ** (-0.5)).reshape(seq_dev, heads_dev, key_dim)
    key_new = (key_sum * inv_rms).reshape(seq_dev, heads_dev, key_dim)
    log_decay = (jax.nn.log_sigmoid(decay_sum * inv_rms) / GATE_NORM).reshape(
        seq_dev, heads_dev, key_dim
    )
    scores, carried, own = front_part(
        query, key_new, log_decay, state, cache_keys, cache_rates, lengths
    )
    return (inv_rms, scores, carried, own)


def close_heads(opened, value_sum, gate_sum, cache_values, head_gain):
    inv_rms, scores, carried, own = opened
    seq_dev, heads_dev, value_dim = carried.shape
    value_new = (value_sum * inv_rms).reshape(seq_dev, heads_dev, value_dim)
    gate = (gate_sum * inv_rms).reshape(seq_dev, heads_dev, value_dim)
    heads = back_part(scores, carried, own, value_new, cache_values, gate, head_gain)
    return heads.reshape(seq_dev, heads_dev * value_dim)


def plain_shards(
    tokens,
    lengths,
    state,
    cache_keys,
    cache_values,
    cache_rates,
    attn_gain,
    w_query,
    w_key,
    w_value,
    w_gate,
    w_decay,
    head_gain,
    w_out,
    mlp_gain,
    w_mlp_gate,
    w_mlp_up,
    w_mlp_down,
):
    seq_dev, heads_dev, value_dim = (state.shape[0], state.shape[1], state.shape[3])
    width = mlp_gain.shape[0]
    n_kv = lax.axis_size("kv")
    n_tp = lax.axis_size("tp")
    block = lax.all_gather(tokens, "tp", axis=1, tiled=True).astype(jnp.float32)
    squares = jnp.sum(block * block, axis=1)
    scaled = (block * attn_gain.astype(jnp.float32)).astype(jnp.bfloat16)
    query_part = jnp.dot(scaled, w_query, preferred_element_type=jnp.float32)
    key_part = jnp.dot(scaled, w_key, preferred_element_type=jnp.float32)
    decay_part = jnp.dot(scaled, w_decay, preferred_element_type=jnp.float32)
    value_part = jnp.dot(scaled, w_value, preferred_element_type=jnp.float32)
    gate_part = jnp.dot(scaled, w_gate, preferred_element_type=jnp.float32)
    every_square = lax.psum(squares, "kv")
    own_squares = lax.dynamic_slice_in_dim(every_square, lax.axis_index("kv") * seq_dev, seq_dev)
    query_sum, key_sum, decay_sum, value_sum, gate_sum = (
        lax.psum_scatter(query_part, "kv", scatter_dimension=0, tiled=True),
        lax.psum_scatter(key_part, "kv", scatter_dimension=0, tiled=True),
        lax.psum_scatter(decay_part, "kv", scatter_dimension=0, tiled=True),
        lax.psum_scatter(value_part, "kv", scatter_dimension=0, tiled=True),
        lax.psum_scatter(gate_part, "kv", scatter_dimension=0, tiled=True),
    )
    opened = open_heads(
        query_sum, key_sum, decay_sum, own_squares, width, state, cache_keys, cache_rates, lengths
    )
    heads = close_heads(opened, value_sum, gate_sum, cache_values, head_gain)
    columns = w_out.shape[1]
    stacked = w_out.reshape(n_tp, heads_dev * value_dim, columns)
    piece = lax.all_gather(
        heads.reshape(1, seq_dev, heads_dev * value_dim), ("kv", "tp"), axis=0, tiled=True
    )
    terms = jnp.einsum("psk,tkc->ptsc", piece, stacked, preferred_element_type=jnp.float32)
    owner = jnp.arange(piece.shape[0], dtype=jnp.int32)
    row_match = (owner // n_tp)[:, None, None] == jnp.arange(n_kv, dtype=jnp.int32)[None, :, None]
    head_match = (owner % n_tp)[:, None, None] == jnp.arange(n_tp, dtype=jnp.int32)[None, None, :]
    chosen = (row_match & head_match).astype(jnp.float32)
    projected = jnp.einsum("prt,ptsc->rsc", chosen, terms, precision=exact_mode)
    projected = projected.reshape(n_kv * seq_dev, columns)
    after = (tokens.astype(jnp.float32) + projected).astype(jnp.bfloat16)
    whole = lax.all_gather(after, ("kv", "tp"), axis=1, tiled=True).astype(jnp.float32)
    inv_second = lax.rsqrt(jnp.mean(whole * whole, axis=1, keepdims=True) + EPS)
    normed = (whole * inv_second * mlp_gain.astype(jnp.float32)).astype(jnp.bfloat16)
    gate_ff = jnp.dot(normed, w_mlp_gate, preferred_element_type=jnp.float32)
    up_ff = jnp.dot(normed, w_mlp_up, preferred_element_type=jnp.float32)
    hidden = (jax.nn.silu(gate_ff) * up_ff).astype(jnp.bfloat16)
    terms = jnp.dot(hidden, w_mlp_down, preferred_element_type=jnp.float32)
    own_share = lax.psum_scatter(terms, ("kv", "tp"), scatter_dimension=1, tiled=True)
    return (after.astype(jnp.float32) + own_share).astype(jnp.bfloat16)


F32 = jnp.float32
BF16 = jnp.bfloat16
LANES = 128


def in_vmem(array):
    return pltpu.with_memory_space_constraint(array, pltpu.VMEM)


def in_hbm(array):
    return pltpu.with_memory_space_constraint(array, pltpu.HBM)


def vmem_spec():
    return pl.BlockSpec(memory_space=pltpu.VMEM)


def call(kernel, out_shape, in_specs, scratch, limit, flops, moved, name):
    return pl.pallas_call(
        kernel,
        out_shape=out_shape,
        in_specs=in_specs,
        out_specs=jax.tree.map(lambda _: vmem_spec(), out_shape),
        scratch_shapes=scratch,
        compiler_params=pltpu.CompilerParams(vmem_limit_bytes=limit),
        cost_estimate=pl.CostEstimate(flops=flops, bytes_accessed=moved, transcendentals=0),
        name=name,
    )


def project_kernel(
    seq_dev, own_ref, other_ref, gain_ref, wq, wk, wd, wv, wg, send_ref, bq, bk, bd, bv, bg, acc, sems
):
    pairs = ((wq, bq), (wk, bk), (wd, bd), (wv, bv), (wg, bg))
    copies = [pltpu.make_async_copy(src, dst, sems.at[i]) for i, (src, dst) in enumerate(pairs)]
    for copy in copies:
        copy.start()
    own = own_ref[...].astype(F32)
    other = other_ref[...].astype(F32)
    first = lax.axis_index("tp") == 0
    low = jnp.where(first, own, other)
    high = jnp.where(first, other, own)
    block = jnp.concatenate([low, high], axis=1)
    total = jnp.sum(block * block, axis=1, keepdims=True)
    scaled = (block * gain_ref[...].astype(F32)).astype(BF16)
    at = 0
    for copy, (_, buf) in zip(copies, pairs):
        copy.wait()
        acc[:, at : at + buf.shape[1]] = jnp.dot(scaled, buf[...], preferred_element_type=F32)
        at += buf.shape[1]
    lane = lax.broadcasted_iota(jnp.int32, (block.shape[0], LANES), 1)
    upper = total.astype(BF16).astype(F32)
    lower = total - upper
    acc[:, at : at + LANES] = jnp.where(lane == 0, upper, jnp.where(lane == 1, lower, 0.0))
    for i in range(send_ref.shape[0]):
        send_ref[i] = acc[i * seq_dev : (i + 1) * seq_dev, :].astype(BF16)


def split_rows(row):
    upper = row.astype(BF16).astype(F32)
    lower = row - upper
    shape = (8, row.shape[1])
    at = lax.broadcasted_iota(jnp.int32, shape, 0)
    upper = jnp.broadcast_to(upper, shape)
    lower = jnp.broadcast_to(lower, shape)
    return jnp.where(at == 0, upper, jnp.where(at == 1, lower, 0.0)).astype(BF16)


def attend_kernel(
    width, lengths_ref, recv_ref, state_ref, keys_ref, values_ref, rates_ref, gain_ref, out_ref, heads_ref
):
    seq_dev, heads_dev, key_dim, value_dim = state_ref.shape
    span = keys_ref.shape[2]
    got = recv_ref[0].astype(F32)
    for i in range(1, recv_ref.shape[0]):
        got = got + recv_ref[i].astype(F32)
    keys_all, values_all = heads_dev * key_dim, heads_dev * value_dim
    ends = [0, keys_all, 2 * keys_all, 3 * keys_all]
    ends += [ends[3] + values_all, ends[3] + 2 * values_all]
    squares = jnp.sum(got[:, ends[5] :], axis=1, keepdims=True)
    inv_rms = lax.rsqrt(squares / width + EPS)
    query = got[:, ends[0] : ends[1]] * inv_rms * key_dim ** (-0.5)
    key_new = got[:, ends[1] : ends[2]] * inv_rms
    raw = got[:, ends[2] : ends[3]] * inv_rms
    log_decay = (jnp.minimum(raw, 0.0) - jnp.log(1.0 + jnp.exp(-jnp.abs(raw)))) / GATE_NORM
    value_new = got[:, ends[3] : ends[4]] * inv_rms
    gate = got[:, ends[4] : ends[5]] * inv_rms
    decayed = query * jnp.exp(log_decay)
    product = query * key_new
    row_at = lax.broadcasted_iota(jnp.int32, (span, span), 0)
    col_at = lax.broadcasted_iota(jnp.int32, (span, span), 1)
    later = jnp.where(col_at > row_at, 1.0, 0.0).astype(BF16)
    slot_col = lax.broadcasted_iota(jnp.int32, (span, 1), 0)
    slot_row = lax.broadcasted_iota(jnp.int32, (1, span), 1)
    for s in range(seq_dev):
        live_col = (slot_col < lengths_ref[s]).astype(F32)
        live_row = (slot_row < lengths_ref[s]).astype(F32)
        for h in range(heads_dev):
            ks, vs = slice(h * key_dim, (h + 1) * key_dim), slice(h * value_dim, (h + 1) * value_dim)
            rates = rates_ref[s, h] * live_col
            upper = rates.astype(BF16)
            lower = (rates - upper.astype(F32)).astype(BF16)
            after = jnp.dot(later, upper, preferred_element_type=F32)
            after = after + jnp.dot(later, lower, preferred_element_type=F32)
            total = jnp.sum(rates, axis=0, keepdims=True)
            weighted = jnp.exp(-after) * keys_ref[s, h].astype(F32)
            w_upper = weighted.astype(BF16)
            w_lower = (weighted - w_upper.astype(F32)).astype(BF16)
            row = decayed[s : s + 1, ks]
            rows = split_rows(row)
            contract = (((1,), (1,)), ((), ()))
            scores = lax.dot_general(rows, w_upper, contract, preferred_element_type=F32)
            scores = scores + lax.dot_general(rows, w_lower, contract, preferred_element_type=F32)
            scores = jnp.sum(scores, axis=0, keepdims=True) * live_row
            state_rows = split_rows(row * jnp.exp(-total))
            mixed = jnp.dot(state_rows, state_ref[s, h].astype(BF16), preferred_element_type=F32)
            mixed = mixed + jnp.dot(split_rows(scores), values_ref[s, h], preferred_element_type=F32)
            own = jnp.sum(product[s : s + 1, ks], axis=1, keepdims=True)
            attended = jnp.sum(mixed, axis=0, keepdims=True) + own * value_new[s : s + 1, vs]
            scale = lax.rsqrt(jnp.mean(attended * attended, axis=1, keepdims=True) + EPS)
            normed = attended * scale * gain_ref[h : h + 1, :].astype(F32)
            opened = gate[s : s + 1, vs]
            heads_ref[s : s + 1, vs] = opened / (1.0 + jnp.exp(-opened)) * normed
    heads = heads_ref[...].astype(BF16)
    for i in range(out_ref.shape[0]):
        out_ref[i] = heads


def output_kernel(n_tp, recv_ref, weight_ref, own_ref, out_ref, rows_ref):
    seq_dev, wide = recv_ref.shape[1], recv_ref.shape[2]
    for i in range(recv_ref.shape[0]):
        kv_at, tp_at = divmod(i, n_tp)
        rows_ref[kv_at * seq_dev : (kv_at + 1) * seq_dev, tp_at * wide : (tp_at + 1) * wide] = recv_ref[
            i
        ].astype(F32)
    projected = jnp.dot(rows_ref[...].astype(BF16), weight_ref[...], preferred_element_type=F32)
    after = (own_ref[...].astype(F32) + projected).astype(BF16)
    for i in range(out_ref.shape[0]):
        out_ref[i] = after


def feed_kernel(recv_ref, gain_ref, gate_ref, up_ref, down_ref, out_ref):
    whole = jnp.concatenate([recv_ref[i].astype(F32) for i in range(recv_ref.shape[0])], axis=1)
    inv = lax.rsqrt(jnp.mean(whole * whole, axis=1, keepdims=True) + EPS)
    normed = (whole * inv * gain_ref[...].astype(F32)).astype(BF16)
    contract = (((1,), (1,)), ((), ()))
    gate = lax.dot_general(normed, gate_ref[...], contract, preferred_element_type=F32)
    up = lax.dot_general(normed, up_ref[...], contract, preferred_element_type=F32)
    hidden = (gate / (1.0 + jnp.exp(-gate)) * up).astype(BF16)
    columns = out_ref.shape[2]
    for i in range(out_ref.shape[0]):
        piece = down_ref[:, i * columns : (i + 1) * columns]
        out_ref[i] = jnp.dot(hidden, piece, preferred_element_type=F32).astype(BF16)


def finish_kernel(recv_ref, after_ref, out_ref):
    total = after_ref[0].astype(F32)
    for i in range(recv_ref.shape[0]):
        total = total + recv_ref[i].astype(F32)
    out_ref[...] = total.astype(BF16)


MIB = 1 << 20


def shards(
    tokens,
    lengths,
    state,
    cache_keys,
    cache_values,
    cache_rates,
    attn_gain,
    w_query,
    w_key,
    w_value,
    w_gate,
    w_decay,
    head_gain,
    w_out,
    mlp_gain,
    w_mlp_gate,
    w_mlp_up,
    w_mlp_down,
):
    seq_dev, heads_dev, key_dim, value_dim = state.shape
    width = mlp_gain.shape[0]
    n_kv, n_tp = lax.axis_size("kv"), lax.axis_size("tp")
    members = n_kv * n_tp
    rows, columns = tokens.shape
    other = lax.ppermute(tokens, "tp", [(i, n_tp - 1 - i) for i in range(n_tp)])
    wide = heads_dev * (3 * key_dim + 2 * value_dim) + LANES
    anywhere = pl.BlockSpec(memory_space=pl.ANY)
    weights = (w_query, w_key, w_decay, w_value, w_gate)
    moved = sum(w.size for w in weights) * 2
    send = call(
        lambda *refs: project_kernel(seq_dev, *refs),
        jax.ShapeDtypeStruct((n_kv, seq_dev, wide), BF16),
        [vmem_spec()] * 3 + [anywhere] * 5,
        [pltpu.VMEM(w.shape, BF16) for w in weights]
        + [pltpu.VMEM((rows, wide), F32), pltpu.SemaphoreType.DMA((5,))],
        16 * MIB,
        rows * moved,
        moved,
        "project",
    )(tokens, other, attn_gain.reshape(1, -1), *(in_hbm(w) for w in weights))
    recv = lax.all_to_all(send, "kv", 0, 0, tiled=True)
    moved = state.size * 4 + cache_rates.size * 8
    send = call(
        lambda *refs: attend_kernel(width, *refs),
        jax.ShapeDtypeStruct((members, seq_dev, heads_dev * value_dim), BF16),
        [pl.BlockSpec(memory_space=pltpu.SMEM)] + [vmem_spec()] * 6,
        [pltpu.VMEM((seq_dev, heads_dev * value_dim), F32)],
        4 * MIB,
        state.size * 16,
        moved,
        "attend",
    )(lengths, recv, in_vmem(state), in_vmem(cache_keys), in_vmem(cache_values), in_vmem(cache_rates), head_gain)
    recv = lax.all_to_all(send, ("kv", "tp"), 0, 0, tiled=True)
    after = call(
        lambda *refs: output_kernel(n_tp, *refs),
        jax.ShapeDtypeStruct((members, rows, columns), BF16),
        [vmem_spec()] * 3,
        [pltpu.VMEM((rows, w_out.shape[0]), F32)],
        2 * MIB,
        rows * w_out.size * 2,
        w_out.size * 2,
        "output",
    )(recv, in_vmem(w_out), tokens)
    recv = lax.all_to_all(after, ("kv", "tp"), 0, 0, tiled=True)
    moved = (w_mlp_gate.size + w_mlp_up.size + w_mlp_down.size) * 2
    send = call(
        feed_kernel,
        jax.ShapeDtypeStruct((members, rows, columns), BF16),
        [vmem_spec()] * 5,
        [],
        4 * MIB,
        rows * moved,
        moved,
        "feed",
    )(recv, mlp_gain.reshape(1, -1), in_vmem(w_mlp_gate.T), in_vmem(w_mlp_up.T), in_vmem(w_mlp_down))
    recv = lax.all_to_all(send, ("kv", "tp"), 0, 0, tiled=True)
    return call(
        finish_kernel,
        jax.ShapeDtypeStruct((rows, columns), BF16),
        [vmem_spec()] * 2,
        [],
        2 * MIB,
        rows * columns * members,
        rows * columns * members * 2,
        "finish",
    )(recv, after)


def solution(mesh):
    placed = (
        P("dp", ("kv", "tp")),
        P(("dp", "kv")),
        P(("dp", "kv"), "tp", None, None),
        P(("dp", "kv"), "tp", None, None),
        P(("dp", "kv"), "tp", None, None),
        P(("dp", "kv"), "tp", None, None),
        P("kv"),
        P("kv", "tp"),
        P("kv", "tp"),
        P("kv", "tp"),
        P("kv", "tp"),
        P("kv", "tp"),
        P("tp", None),
        P(None, ("kv", "tp")),
        P(),
        P(None, ("kv", "tp")),
        P(None, ("kv", "tp")),
        P(("kv", "tp"), None),
    )
    sizes = mesh.shape

    def body(*args):
        fits = sizes["tp"] == 2 and args[13].shape[1] % LANES == 0
        return (shards if fits else plain_shards)(*args)

    return jax.shard_map(
        body, mesh=mesh, in_specs=placed, out_specs=P("dp", ("kv", "tp")), check_vma=False
    )
```

```python
import jax
import jax.numpy as jnp
from jax import lax
from jax.experimental import pallas as pl
from jax.experimental.pallas import tpu as pltpu
from jax.sharding import PartitionSpec as P

EPS = 1e-06
GATE_NORM = 16.0
exact_mode = lax.Precision.HIGHEST


def front_part(query, key_new, log_decay, state, cache_keys, cache_rates, lengths):
    span = cache_keys.shape[2]
    live = (jnp.arange(span, dtype=jnp.int32)[None, :] < lengths[:, None]).astype(jnp.float32)
    running = jnp.cumsum(cache_rates * live[:, None, :, None], axis=2)
    total = running[:, :, -1:, :]
    weight = jnp.exp(running - total + log_decay[:, :, None, :])
    scores = (
        jnp.einsum(
            "bhd,bhjd->bhj", query, weight * cache_keys.astype(jnp.float32), precision=exact_mode
        )
        * live[:, None, :]
    )
    carried = jnp.einsum(
        "bhd,bhde->bhe", query * jnp.exp(log_decay - total[:, :, 0, :]), state, precision=exact_mode
    )
    own = jnp.sum(query * key_new, axis=-1, keepdims=True)
    return (scores, carried, own)


def back_part(scores, carried, own, value_new, cache_values, gate, head_gain):
    inner = jnp.einsum(
        "bhj,bhje->bhe", scores, cache_values.astype(jnp.float32), precision=exact_mode
    )
    attended = carried + inner + own * value_new
    normed = attended * lax.rsqrt(jnp.mean(attended * attended, axis=-1, keepdims=True) + EPS)
    normed = normed * head_gain.astype(jnp.float32)
    return (jax.nn.silu(gate) * normed).astype(jnp.bfloat16)


def open_heads(
    query_sum, key_sum, decay_sum, own_squares, width, state, cache_keys, cache_rates, lengths
):
    seq_dev, heads_dev, key_dim = (state.shape[0], state.shape[1], state.shape[2])
    inv_rms = lax.rsqrt(own_squares / width + EPS)[:, None]
    query = (query_sum * inv_rms * key_dim ** (-0.5)).reshape(seq_dev, heads_dev, key_dim)
    key_new = (key_sum * inv_rms).reshape(seq_dev, heads_dev, key_dim)
    log_decay = (jax.nn.log_sigmoid(decay_sum * inv_rms) / GATE_NORM).reshape(
        seq_dev, heads_dev, key_dim
    )
    scores, carried, own = front_part(
        query, key_new, log_decay, state, cache_keys, cache_rates, lengths
    )
    return (inv_rms, scores, carried, own)


def close_heads(opened, value_sum, gate_sum, cache_values, head_gain):
    inv_rms, scores, carried, own = opened
    seq_dev, heads_dev, value_dim = carried.shape
    value_new = (value_sum * inv_rms).reshape(seq_dev, heads_dev, value_dim)
    gate = (gate_sum * inv_rms).reshape(seq_dev, heads_dev, value_dim)
    heads = back_part(scores, carried, own, value_new, cache_values, gate, head_gain)
    return heads.reshape(seq_dev, heads_dev * value_dim)


def plain_shards(
    tokens,
    lengths,
    state,
    cache_keys,
    cache_values,
    cache_rates,
    attn_gain,
    w_query,
    w_key,
    w_value,
    w_gate,
    w_decay,
    head_gain,
    w_out,
    mlp_gain,
    w_mlp_gate,
    w_mlp_up,
    w_mlp_down,
):
    seq_dev, heads_dev, value_dim = (state.shape[0], state.shape[1], state.shape[3])
    width = mlp_gain.shape[0]
    n_kv = lax.axis_size("kv")
    n_tp = lax.axis_size("tp")
    block = lax.all_gather(tokens, "tp", axis=1, tiled=True).astype(jnp.float32)
    squares = jnp.sum(block * block, axis=1)
    scaled = (block * attn_gain.astype(jnp.float32)).astype(jnp.bfloat16)
    query_part = jnp.dot(scaled, w_query, preferred_element_type=jnp.float32)
    key_part = jnp.dot(scaled, w_key, preferred_element_type=jnp.float32)
    decay_part = jnp.dot(scaled, w_decay, preferred_element_type=jnp.float32)
    value_part = jnp.dot(scaled, w_value, preferred_element_type=jnp.float32)
    gate_part = jnp.dot(scaled, w_gate, preferred_element_type=jnp.float32)
    every_square = lax.psum(squares, "kv")
    own_squares = lax.dynamic_slice_in_dim(every_square, lax.axis_index("kv") * seq_dev, seq_dev)
    query_sum, key_sum, decay_sum, value_sum, gate_sum = (
        lax.psum_scatter(query_part, "kv", scatter_dimension=0, tiled=True),
        lax.psum_scatter(key_part, "kv", scatter_dimension=0, tiled=True),
        lax.psum_scatter(decay_part, "kv", scatter_dimension=0, tiled=True),
        lax.psum_scatter(value_part, "kv", scatter_dimension=0, tiled=True),
        lax.psum_scatter(gate_part, "kv", scatter_dimension=0, tiled=True),
    )
    opened = open_heads(
        query_sum, key_sum, decay_sum, own_squares, width, state, cache_keys, cache_rates, lengths
    )
    heads = close_heads(opened, value_sum, gate_sum, cache_values, head_gain)
    columns = w_out.shape[1]
    stacked = w_out.reshape(n_tp, heads_dev * value_dim, columns)
    piece = lax.all_gather(
        heads.reshape(1, seq_dev, heads_dev * value_dim), ("kv", "tp"), axis=0, tiled=True
    )
    terms = jnp.einsum("psk,tkc->ptsc", piece, stacked, preferred_element_type=jnp.float32)
    owner = jnp.arange(piece.shape[0], dtype=jnp.int32)
    row_match = (owner // n_tp)[:, None, None] == jnp.arange(n_kv, dtype=jnp.int32)[None, :, None]
    head_match = (owner % n_tp)[:, None, None] == jnp.arange(n_tp, dtype=jnp.int32)[None, None, :]
    chosen = (row_match & head_match).astype(jnp.float32)
    projected = jnp.einsum("prt,ptsc->rsc", chosen, terms, precision=exact_mode)
    projected = projected.reshape(n_kv * seq_dev, columns)
    after = (tokens.astype(jnp.float32) + projected).astype(jnp.bfloat16)
    whole = lax.all_gather(after, ("kv", "tp"), axis=1, tiled=True).astype(jnp.float32)
    inv_second = lax.rsqrt(jnp.mean(whole * whole, axis=1, keepdims=True) + EPS)
    normed = (whole * inv_second * mlp_gain.astype(jnp.float32)).astype(jnp.bfloat16)
    gate_ff = jnp.dot(normed, w_mlp_gate, preferred_element_type=jnp.float32)
    up_ff = jnp.dot(normed, w_mlp_up, preferred_element_type=jnp.float32)
    hidden = (jax.nn.silu(gate_ff) * up_ff).astype(jnp.bfloat16)
    terms = jnp.dot(hidden, w_mlp_down, preferred_element_type=jnp.float32)
    own_share = lax.psum_scatter(terms, ("kv", "tp"), scatter_dimension=1, tiled=True)
    return (after.astype(jnp.float32) + own_share).astype(jnp.bfloat16)


F32 = jnp.float32
BF16 = jnp.bfloat16
LANES = 128


def in_vmem(array):
    return pltpu.with_memory_space_constraint(array, pltpu.VMEM)


def in_hbm(array):
    return pltpu.with_memory_space_constraint(array, pltpu.HBM)


def vmem_spec():
    return pl.BlockSpec(memory_space=pltpu.VMEM)


def call(kernel, out_shape, in_specs, scratch, limit, flops, moved, name):
    return pl.pallas_call(
        kernel,
        out_shape=out_shape,
        in_specs=in_specs,
        out_specs=jax.tree.map(lambda _: vmem_spec(), out_shape),
        scratch_shapes=scratch,
        compiler_params=pltpu.CompilerParams(vmem_limit_bytes=limit),
        cost_estimate=pl.CostEstimate(flops=flops, bytes_accessed=moved, transcendentals=0),
        name=name,
    )


def spread(gain_ref):
    rows = gain_ref[...].astype(F32)
    return jnp.concatenate([rows[i : i + 1] for i in range(rows.shape[0])], axis=1)


def project_kernel(
    seq_dev, own_hbm, other_ref, gain_hbm, wq, wk, wd, wv, wg, send_ref, own_ref, gain_ref, bq, bk, bd, bv, bg, acc, sems
):
    pairs = ((own_hbm, own_ref), (gain_hbm, gain_ref), (wq, bq), (wk, bk), (wd, bd), (wv, bv), (wg, bg))
    copies = [pltpu.make_async_copy(src, dst, sems.at[i]) for i, (src, dst) in enumerate(pairs)]
    for copy in copies:
        copy.start()
    copies[0].wait()
    copies[1].wait()
    own = own_ref[...].astype(F32)
    other = other_ref[...].astype(F32)
    first = lax.axis_index("tp") == 0
    low = jnp.where(first, own, other)
    high = jnp.where(first, other, own)
    block = jnp.concatenate([low, high], axis=1)
    total = jnp.sum(block * block, axis=1, keepdims=True)
    scaled = (block * spread(gain_ref)).astype(BF16)
    at = 0
    for copy, (_, buf) in zip(copies[2:], pairs[2:]):
        copy.wait()
        acc[:, at : at + buf.shape[1]] = jnp.dot(scaled, buf[...], preferred_element_type=F32)
        at += buf.shape[1]
    lane = lax.broadcasted_iota(jnp.int32, (block.shape[0], LANES), 1)
    upper = total.astype(BF16).astype(F32)
    lower = total - upper
    acc[:, at : at + LANES] = jnp.where(lane == 0, upper, jnp.where(lane == 1, lower, 0.0))
    for i in range(send_ref.shape[0]):
        send_ref[i] = acc[i * seq_dev : (i + 1) * seq_dev, :].astype(BF16)


def split_rows(row):
    upper = row.astype(BF16).astype(F32)
    lower = row - upper
    shape = (8, row.shape[1])
    at = lax.broadcasted_iota(jnp.int32, shape, 0)
    upper = jnp.broadcast_to(upper, shape)
    lower = jnp.broadcast_to(lower, shape)
    return jnp.where(at == 0, upper, jnp.where(at == 1, lower, 0.0)).astype(BF16)


def attend_kernel(
    width, lengths_ref, recv_ref, state_ref, keys_ref, values_ref, rates_ref, gain_ref, out_ref, heads_ref
):
    seq_dev, heads_dev, key_dim, value_dim = state_ref.shape
    span = keys_ref.shape[2]
    got = recv_ref[0].astype(F32)
    for i in range(1, recv_ref.shape[0]):
        got = got + recv_ref[i].astype(F32)
    keys_all, values_all = heads_dev * key_dim, heads_dev * value_dim
    ends = [0, keys_all, 2 * keys_all, 3 * keys_all]
    ends += [ends[3] + values_all, ends[3] + 2 * values_all]
    squares = jnp.sum(got[:, ends[5] :], axis=1, keepdims=True)
    inv_rms = lax.rsqrt(squares / width + EPS)
    query = got[:, ends[0] : ends[1]] * inv_rms * key_dim ** (-0.5)
    key_new = got[:, ends[1] : ends[2]] * inv_rms
    raw = got[:, ends[2] : ends[3]] * inv_rms
    log_decay = (jnp.minimum(raw, 0.0) - jnp.log(1.0 + jnp.exp(-jnp.abs(raw)))) / GATE_NORM
    value_new = got[:, ends[3] : ends[4]] * inv_rms
    gate = got[:, ends[4] : ends[5]] * inv_rms
    decayed = query * jnp.exp(log_decay)
    product = query * key_new
    row_at = lax.broadcasted_iota(jnp.int32, (span, span), 0)
    col_at = lax.broadcasted_iota(jnp.int32, (span, span), 1)
    later = jnp.where(col_at > row_at, 1.0, 0.0).astype(BF16)
    slot_col = lax.broadcasted_iota(jnp.int32, (span, 1), 0)
    slot_row = lax.broadcasted_iota(jnp.int32, (1, span), 1)
    for s in range(seq_dev):
        live_col = (slot_col < lengths_ref[s]).astype(F32)
        live_row = (slot_row < lengths_ref[s]).astype(F32)
        for h in range(heads_dev):
            ks, vs = slice(h * key_dim, (h + 1) * key_dim), slice(h * value_dim, (h + 1) * value_dim)
            rates = rates_ref[s, h] * live_col
            upper = rates.astype(BF16)
            lower = (rates - upper.astype(F32)).astype(BF16)
            after = jnp.dot(later, upper, preferred_element_type=F32)
            after = after + jnp.dot(later, lower, preferred_element_type=F32)
            total = jnp.sum(rates, axis=0, keepdims=True)
            weighted = jnp.exp(-after) * keys_ref[s, h].astype(F32)
            w_upper = weighted.astype(BF16)
            w_lower = (weighted - w_upper.astype(F32)).astype(BF16)
            row = decayed[s : s + 1, ks]
            rows = split_rows(row)
            contract = (((1,), (1,)), ((), ()))
            scores = lax.dot_general(rows, w_upper, contract, preferred_element_type=F32)
            scores = scores + lax.dot_general(rows, w_lower, contract, preferred_element_type=F32)
            scores = jnp.sum(scores, axis=0, keepdims=True) * live_row
            state_rows = split_rows(row * jnp.exp(-total))
            mixed = jnp.dot(state_rows, state_ref[s, h].astype(BF16), preferred_element_type=F32)
            mixed = mixed + jnp.dot(split_rows(scores), values_ref[s, h], preferred_element_type=F32)
            own = jnp.sum(product[s : s + 1, ks], axis=1, keepdims=True)
            attended = jnp.sum(mixed, axis=0, keepdims=True) + own * value_new[s : s + 1, vs]
            scale = lax.rsqrt(jnp.mean(attended * attended, axis=1, keepdims=True) + EPS)
            normed = attended * scale * gain_ref[h : h + 1, :].astype(F32)
            opened = gate[s : s + 1, vs]
            heads_ref[s : s + 1, vs] = opened / (1.0 + jnp.exp(-opened)) * normed
    heads = heads_ref[...].astype(BF16)
    for i in range(out_ref.shape[0]):
        out_ref[i] = heads


def output_kernel(n_tp, recv_ref, weight_ref, own_ref, out_ref, after_ref, rows_ref):
    seq_dev, wide = recv_ref.shape[1], recv_ref.shape[2]
    for i in range(recv_ref.shape[0]):
        kv_at, tp_at = divmod(i, n_tp)
        rows_ref[kv_at * seq_dev : (kv_at + 1) * seq_dev, tp_at * wide : (tp_at + 1) * wide] = recv_ref[
            i
        ].astype(F32)
    projected = jnp.dot(rows_ref[...].astype(BF16), weight_ref[...], preferred_element_type=F32)
    after = (own_ref[...].astype(F32) + projected).astype(BF16)
    after_ref[...] = after
    for i in range(out_ref.shape[0]):
        out_ref[i] = after


def feed_kernel(recv_ref, gain_ref, gate_ref, up_ref, down_ref, out_ref):
    whole = jnp.concatenate([recv_ref[i].astype(F32) for i in range(recv_ref.shape[0])], axis=1)
    inv = lax.rsqrt(jnp.mean(whole * whole, axis=1, keepdims=True) + EPS)
    normed = (whole * inv * spread(gain_ref)).astype(BF16)
    contract = (((1,), (1,)), ((), ()))
    gate = lax.dot_general(normed, gate_ref[...], contract, preferred_element_type=F32)
    up = lax.dot_general(normed, up_ref[...], contract, preferred_element_type=F32)
    hidden = (gate / (1.0 + jnp.exp(-gate)) * up).astype(BF16)
    columns = out_ref.shape[2]
    for i in range(out_ref.shape[0]):
        piece = down_ref[:, i * columns : (i + 1) * columns]
        out_ref[i] = jnp.dot(hidden, piece, preferred_element_type=F32).astype(BF16)


def finish_kernel(recv_ref, after_ref, out_ref):
    total = after_ref[...].astype(F32)
    for i in range(recv_ref.shape[0]):
        total = total + recv_ref[i].astype(F32)
    out_ref[...] = total.astype(BF16)


MIB = 1 << 20


def shards(
    tokens,
    lengths,
    state,
    cache_keys,
    cache_values,
    cache_rates,
    attn_gain,
    w_query,
    w_key,
    w_value,
    w_gate,
    w_decay,
    head_gain,
    w_out,
    mlp_gain,
    w_mlp_gate,
    w_mlp_up,
    w_mlp_down,
):
    seq_dev, heads_dev, key_dim, value_dim = state.shape
    width = mlp_gain.shape[0]
    n_kv, n_tp = lax.axis_size("kv"), lax.axis_size("tp")
    members = n_kv * n_tp
    rows, columns = tokens.shape
    other = lax.ppermute(tokens, "tp", [(i, n_tp - 1 - i) for i in range(n_tp)])
    wide = heads_dev * (3 * key_dim + 2 * value_dim) + LANES
    anywhere = pl.BlockSpec(memory_space=pl.ANY)
    weights = (w_query, w_key, w_decay, w_value, w_gate)
    moved = sum(w.size for w in weights) * 2
    send = call(
        lambda *refs: project_kernel(seq_dev, *refs),
        jax.ShapeDtypeStruct((n_kv, seq_dev, wide), BF16),
        [anywhere, vmem_spec()] + [anywhere] * 6,
        [pltpu.VMEM(tokens.shape, BF16), pltpu.VMEM((attn_gain.size // LANES, LANES), BF16)]
        + [pltpu.VMEM(w.shape, BF16) for w in weights]
        + [pltpu.VMEM((rows, wide), F32), pltpu.SemaphoreType.DMA((7,))],
        16 * MIB,
        10**10,
        moved,
        "project",
    )(in_hbm(tokens), other, in_hbm(attn_gain.reshape(-1, LANES)), *(in_hbm(w) for w in weights))
    recv = lax.all_to_all(send, "kv", 0, 0, tiled=True)
    moved = state.size * 4 + cache_rates.size * 8
    send = call(
        lambda *refs: attend_kernel(width, *refs),
        jax.ShapeDtypeStruct((members, seq_dev, heads_dev * value_dim), BF16),
        [pl.BlockSpec(memory_space=pltpu.SMEM)] + [vmem_spec()] * 6,
        [pltpu.VMEM((seq_dev, heads_dev * value_dim), F32)],
        4 * MIB,
        4 * 10**10,
        moved,
        "attend",
    )(lengths, recv, in_vmem(state), in_vmem(cache_keys), in_vmem(cache_values), in_vmem(cache_rates), in_vmem(head_gain))
    recv = lax.all_to_all(send, ("kv", "tp"), 0, 0, tiled=True)
    send, after = call(
        lambda *refs: output_kernel(n_tp, *refs),
        (jax.ShapeDtypeStruct((members, rows, columns), BF16), jax.ShapeDtypeStruct((rows, columns), BF16)),
        [vmem_spec()] * 3,
        [pltpu.VMEM((rows, w_out.shape[0]), F32)],
        2 * MIB,
        10**6,
        w_out.size * 2,
        "output",
    )(recv, in_vmem(w_out), in_vmem(tokens))
    recv = lax.all_to_all(send, ("kv", "tp"), 0, 0, tiled=True)
    moved = (w_mlp_gate.size + w_mlp_up.size + w_mlp_down.size) * 2
    send = call(
        feed_kernel,
        jax.ShapeDtypeStruct((members, rows, columns), BF16),
        [vmem_spec()] * 5,
        [],
        4 * MIB,
        rows * moved,
        moved,
        "feed",
    )(recv, in_vmem(mlp_gain.reshape(-1, LANES)), in_vmem(w_mlp_gate.T), in_vmem(w_mlp_up.T), in_vmem(w_mlp_down))
    recv = lax.all_to_all(send, ("kv", "tp"), 0, 0, tiled=True)
    return call(
        finish_kernel,
        jax.ShapeDtypeStruct((rows, columns), BF16),
        [vmem_spec()] * 2,
        [],
        2 * MIB,
        rows * columns * members,
        rows * columns * members * 2,
        "finish",
    )(recv, after)


def solution(mesh):
    placed = (
        P("dp", ("kv", "tp")),
        P(("dp", "kv")),
        P(("dp", "kv"), "tp", None, None),
        P(("dp", "kv"), "tp", None, None),
        P(("dp", "kv"), "tp", None, None),
        P(("dp", "kv"), "tp", None, None),
        P("kv"),
        P("kv", "tp"),
        P("kv", "tp"),
        P("kv", "tp"),
        P("kv", "tp"),
        P("kv", "tp"),
        P("tp", None),
        P(None, ("kv", "tp")),
        P(),
        P(None, ("kv", "tp")),
        P(None, ("kv", "tp")),
        P(("kv", "tp"), None),
    )
    sizes = mesh.shape

    def body(*args):
        fits = sizes["tp"] == 2 and args[13].shape[1] % LANES == 0
        return (shards if fits else plain_shards)(*args)

    return jax.shard_map(
        body, mesh=mesh, in_specs=placed, out_specs=P("dp", ("kv", "tp")), check_vma=False
    )
```

```python
import jax
import jax.numpy as jnp
from jax import lax
from jax.experimental import pallas as pl
from jax.experimental.pallas import tpu as pltpu
from jax.sharding import PartitionSpec as P

EPS = 1e-06
GATE_NORM = 16.0
exact_mode = lax.Precision.HIGHEST


def front_part(query, key_new, log_decay, state, cache_keys, cache_rates, lengths):
    span = cache_keys.shape[2]
    live = (jnp.arange(span, dtype=jnp.int32)[None, :] < lengths[:, None]).astype(jnp.float32)
    running = jnp.cumsum(cache_rates * live[:, None, :, None], axis=2)
    total = running[:, :, -1:, :]
    weight = jnp.exp(running - total + log_decay[:, :, None, :])
    scores = (
        jnp.einsum(
            "bhd,bhjd->bhj", query, weight * cache_keys.astype(jnp.float32), precision=exact_mode
        )
        * live[:, None, :]
    )
    carried = jnp.einsum(
        "bhd,bhde->bhe", query * jnp.exp(log_decay - total[:, :, 0, :]), state, precision=exact_mode
    )
    own = jnp.sum(query * key_new, axis=-1, keepdims=True)
    return (scores, carried, own)


def back_part(scores, carried, own, value_new, cache_values, gate, head_gain):
    inner = jnp.einsum(
        "bhj,bhje->bhe", scores, cache_values.astype(jnp.float32), precision=exact_mode
    )
    attended = carried + inner + own * value_new
    normed = attended * lax.rsqrt(jnp.mean(attended * attended, axis=-1, keepdims=True) + EPS)
    normed = normed * head_gain.astype(jnp.float32)
    return (jax.nn.silu(gate) * normed).astype(jnp.bfloat16)


def open_heads(
    query_sum, key_sum, decay_sum, own_squares, width, state, cache_keys, cache_rates, lengths
):
    seq_dev, heads_dev, key_dim = (state.shape[0], state.shape[1], state.shape[2])
    inv_rms = lax.rsqrt(own_squares / width + EPS)[:, None]
    query = (query_sum * inv_rms * key_dim ** (-0.5)).reshape(seq_dev, heads_dev, key_dim)
    key_new = (key_sum * inv_rms).reshape(seq_dev, heads_dev, key_dim)
    log_decay = (jax.nn.log_sigmoid(decay_sum * inv_rms) / GATE_NORM).reshape(
        seq_dev, heads_dev, key_dim
    )
    scores, carried, own = front_part(
        query, key_new, log_decay, state, cache_keys, cache_rates, lengths
    )
    return (inv_rms, scores, carried, own)


def close_heads(opened, value_sum, gate_sum, cache_values, head_gain):
    inv_rms, scores, carried, own = opened
    seq_dev, heads_dev, value_dim = carried.shape
    value_new = (value_sum * inv_rms).reshape(seq_dev, heads_dev, value_dim)
    gate = (gate_sum * inv_rms).reshape(seq_dev, heads_dev, value_dim)
    heads = back_part(scores, carried, own, value_new, cache_values, gate, head_gain)
    return heads.reshape(seq_dev, heads_dev * value_dim)


def plain_shards(
    tokens,
    lengths,
    state,
    cache_keys,
    cache_values,
    cache_rates,
    attn_gain,
    w_query,
    w_key,
    w_value,
    w_gate,
    w_decay,
    head_gain,
    w_out,
    mlp_gain,
    w_mlp_gate,
    w_mlp_up,
    w_mlp_down,
):
    seq_dev, heads_dev, value_dim = (state.shape[0], state.shape[1], state.shape[3])
    width = mlp_gain.shape[0]
    n_kv = lax.axis_size("kv")
    n_tp = lax.axis_size("tp")
    block = lax.all_gather(tokens, "tp", axis=1, tiled=True).astype(jnp.float32)
    squares = jnp.sum(block * block, axis=1)
    scaled = (block * attn_gain.astype(jnp.float32)).astype(jnp.bfloat16)
    query_part = jnp.dot(scaled, w_query, preferred_element_type=jnp.float32)
    key_part = jnp.dot(scaled, w_key, preferred_element_type=jnp.float32)
    decay_part = jnp.dot(scaled, w_decay, preferred_element_type=jnp.float32)
    value_part = jnp.dot(scaled, w_value, preferred_element_type=jnp.float32)
    gate_part = jnp.dot(scaled, w_gate, preferred_element_type=jnp.float32)
    every_square = lax.psum(squares, "kv")
    own_squares = lax.dynamic_slice_in_dim(every_square, lax.axis_index("kv") * seq_dev, seq_dev)
    query_sum, key_sum, decay_sum, value_sum, gate_sum = (
        lax.psum_scatter(query_part, "kv", scatter_dimension=0, tiled=True),
        lax.psum_scatter(key_part, "kv", scatter_dimension=0, tiled=True),
        lax.psum_scatter(decay_part, "kv", scatter_dimension=0, tiled=True),
        lax.psum_scatter(value_part, "kv", scatter_dimension=0, tiled=True),
        lax.psum_scatter(gate_part, "kv", scatter_dimension=0, tiled=True),
    )
    opened = open_heads(
        query_sum, key_sum, decay_sum, own_squares, width, state, cache_keys, cache_rates, lengths
    )
    heads = close_heads(opened, value_sum, gate_sum, cache_values, head_gain)
    columns = w_out.shape[1]
    stacked = w_out.reshape(n_tp, heads_dev * value_dim, columns)
    piece = lax.all_gather(
        heads.reshape(1, seq_dev, heads_dev * value_dim), ("kv", "tp"), axis=0, tiled=True
    )
    terms = jnp.einsum("psk,tkc->ptsc", piece, stacked, preferred_element_type=jnp.float32)
    owner = jnp.arange(piece.shape[0], dtype=jnp.int32)
    row_match = (owner // n_tp)[:, None, None] == jnp.arange(n_kv, dtype=jnp.int32)[None, :, None]
    head_match = (owner % n_tp)[:, None, None] == jnp.arange(n_tp, dtype=jnp.int32)[None, None, :]
    chosen = (row_match & head_match).astype(jnp.float32)
    projected = jnp.einsum("prt,ptsc->rsc", chosen, terms, precision=exact_mode)
    projected = projected.reshape(n_kv * seq_dev, columns)
    after = (tokens.astype(jnp.float32) + projected).astype(jnp.bfloat16)
    whole = lax.all_gather(after, ("kv", "tp"), axis=1, tiled=True).astype(jnp.float32)
    inv_second = lax.rsqrt(jnp.mean(whole * whole, axis=1, keepdims=True) + EPS)
    normed = (whole * inv_second * mlp_gain.astype(jnp.float32)).astype(jnp.bfloat16)
    gate_ff = jnp.dot(normed, w_mlp_gate, preferred_element_type=jnp.float32)
    up_ff = jnp.dot(normed, w_mlp_up, preferred_element_type=jnp.float32)
    hidden = (jax.nn.silu(gate_ff) * up_ff).astype(jnp.bfloat16)
    terms = jnp.dot(hidden, w_mlp_down, preferred_element_type=jnp.float32)
    own_share = lax.psum_scatter(terms, ("kv", "tp"), scatter_dimension=1, tiled=True)
    return (after.astype(jnp.float32) + own_share).astype(jnp.bfloat16)


F32 = jnp.float32
BF16 = jnp.bfloat16
LANES = 128


def in_vmem(array):
    return pltpu.with_memory_space_constraint(array, pltpu.VMEM)


def in_hbm(array):
    return pltpu.with_memory_space_constraint(array, pltpu.HBM)


def vmem_spec():
    return pl.BlockSpec(memory_space=pltpu.VMEM)


def call(kernel, out_shape, in_specs, scratch, limit, flops, moved, name):
    return pl.pallas_call(
        kernel,
        out_shape=out_shape,
        in_specs=in_specs,
        out_specs=jax.tree.map(lambda _: vmem_spec(), out_shape),
        scratch_shapes=scratch,
        compiler_params=pltpu.CompilerParams(vmem_limit_bytes=limit),
        cost_estimate=pl.CostEstimate(flops=flops, bytes_accessed=moved, transcendentals=0),
        name=name,
    )


def spread(gain_ref):
    rows = gain_ref[...].astype(F32)
    return jnp.concatenate([rows[i : i + 1] for i in range(rows.shape[0])], axis=1)


def by_partner(block, seq_dev, n_kv):
    me = lax.axis_index("kv")
    place = lax.broadcasted_iota(jnp.int32, block.shape, 0) // seq_dev
    rows = block.shape[0]
    bit = 1
    while bit < n_kv:
        down = pltpu.roll(block, bit * seq_dev, 0)
        up = pltpu.roll(block, rows - bit * seq_dev, 0)
        swapped = jnp.where((place & bit) == 0, up, down)
        block = jnp.where((me & bit) == 0, block, swapped)
        bit *= 2
    return block


def project_kernel(
    seq_dev, own_hbm, other_ref, gain_hbm, wq, wk, wd, wv, wg, *rest
):
    out_refs, (own_ref, gain_ref, bq, bk, bd, bv, bg, acc, sems) = rest[:-9], rest[-9:]
    pairs = ((own_hbm, own_ref), (gain_hbm, gain_ref), (wq, bq), (wk, bk), (wd, bd), (wv, bv), (wg, bg))
    copies = [pltpu.make_async_copy(src, dst, sems.at[i]) for i, (src, dst) in enumerate(pairs)]
    for copy in copies:
        copy.start()
    copies[0].wait()
    copies[1].wait()
    own = own_ref[...].astype(F32)
    other = other_ref[...].astype(F32)
    first = lax.axis_index("tp") == 0
    low = jnp.where(first, own, other)
    high = jnp.where(first, other, own)
    block = by_partner(jnp.concatenate([low, high], axis=1), seq_dev, len(out_refs))
    total = jnp.sum(block * block, axis=1, keepdims=True)
    scaled = (block * spread(gain_ref)).astype(BF16)
    at = 0
    for copy, (_, buf) in zip(copies[2:], pairs[2:]):
        copy.wait()
        acc[:, at : at + buf.shape[1]] = jnp.dot(scaled, buf[...], preferred_element_type=F32)
        at += buf.shape[1]
    lane = lax.broadcasted_iota(jnp.int32, (block.shape[0], LANES), 1)
    upper = total.astype(BF16).astype(F32)
    lower = total - upper
    acc[:, at : at + LANES] = jnp.where(lane == 0, upper, jnp.where(lane == 1, lower, 0.0))
    for step, out_ref in enumerate(out_refs):
        out_ref[...] = acc[step * seq_dev : (step + 1) * seq_dev, :].astype(out_ref.dtype)


def split_rows(row):
    upper = row.astype(BF16).astype(F32)
    lower = row - upper
    shape = (8, row.shape[1])
    at = lax.broadcasted_iota(jnp.int32, shape, 0)
    upper = jnp.broadcast_to(upper, shape)
    lower = jnp.broadcast_to(lower, shape)
    return jnp.where(at == 0, upper, jnp.where(at == 1, lower, 0.0)).astype(BF16)


def gather_kernel(lengths_ref, _, state_ref, keys_ref, values_ref, rates_ref, mixed_ref, total_ref):
    seq_dev, heads_dev, key_dim, value_dim = state_ref.shape
    span = keys_ref.shape[2]
    row_at = lax.broadcasted_iota(jnp.int32, (span, span), 0)
    col_at = lax.broadcasted_iota(jnp.int32, (span, span), 1)
    upto = jnp.where(col_at <= row_at, 1.0, 0.0).astype(BF16)
    slot = lax.broadcasted_iota(jnp.int32, (span, 1), 0)
    for s in range(seq_dev):
        live = (slot < lengths_ref[s]).astype(F32)
        for h in range(heads_dev):
            rates = rates_ref[s, h] * live
            upper = rates.astype(BF16)
            lower = (rates - upper.astype(F32)).astype(BF16)
            running = jnp.dot(upto, upper, preferred_element_type=F32)
            running = running + jnp.dot(upto, lower, preferred_element_type=F32)
            total_ref[s : s + 1, h * key_dim : (h + 1) * key_dim] = running[span - 1 :]
            grown = (jnp.exp(running) * keys_ref[s, h].astype(F32) * live).astype(BF16)
            added = lax.dot_general(
                grown, values_ref[s, h], (((0,), (0,)), ((), ())), preferred_element_type=F32
            )
            mixed_ref[s, h] = (state_ref[s, h] + added).astype(BF16)


def attend_kernel(width, parts, mixed_ref, total_ref, gain_ref, out_ref, heads_ref):
    seq_dev, heads_dev, key_dim, value_dim = mixed_ref.shape
    got = parts[0][...]
    for part in parts[1:]:
        got = got + part[...].astype(F32)
    keys_all, values_all = heads_dev * key_dim, heads_dev * value_dim
    ends = [0, keys_all, 2 * keys_all, 3 * keys_all]
    ends += [ends[3] + values_all, ends[3] + 2 * values_all]
    squares = jnp.sum(got[:, ends[5] :], axis=1, keepdims=True)
    inv_rms = lax.rsqrt(squares / width + EPS)
    query = got[:, ends[0] : ends[1]] * inv_rms * key_dim ** (-0.5)
    key_new = got[:, ends[1] : ends[2]] * inv_rms
    raw = got[:, ends[2] : ends[3]] * inv_rms
    log_decay = (jnp.minimum(raw, 0.0) - jnp.log(1.0 + jnp.exp(-jnp.abs(raw)))) / GATE_NORM
    value_new = got[:, ends[3] : ends[4]] * inv_rms
    gate = got[:, ends[4] : ends[5]] * inv_rms
    gate = gate / (1.0 + jnp.exp(-gate))
    decayed = query * jnp.exp(log_decay - total_ref[...])
    product = query * key_new
    for s in range(seq_dev):
        for h in range(heads_dev):
            ks, vs = slice(h * key_dim, (h + 1) * key_dim), slice(h * value_dim, (h + 1) * value_dim)
            rows = split_rows(decayed[s : s + 1, ks])
            mixed = jnp.dot(rows, mixed_ref[s, h], preferred_element_type=F32)
            own = jnp.sum(product[s : s + 1, ks], axis=1, keepdims=True)
            heads_ref[s : s + 1, vs] = jnp.sum(mixed, axis=0, keepdims=True) + own * value_new[s : s + 1, vs]
    pieces = []
    for h in range(heads_dev):
        vs = slice(h * value_dim, (h + 1) * value_dim)
        attended = heads_ref[:, vs]
        scale = lax.rsqrt(jnp.mean(attended * attended, axis=1, keepdims=True) + EPS)
        pieces.append(gate[:, vs] * (attended * scale * gain_ref[h : h + 1, :].astype(F32)))
    heads = jnp.concatenate(pieces, axis=1).astype(BF16)
    for i in range(out_ref.shape[0]):
        out_ref[i] = heads


def output_kernel(n_tp, recv_ref, weight_ref, own_ref, out_ref, after_ref, rows_ref):
    seq_dev, wide = recv_ref.shape[1], recv_ref.shape[2]
    for i in range(recv_ref.shape[0]):
        kv_at, tp_at = divmod(i, n_tp)
        rows_ref[kv_at * seq_dev : (kv_at + 1) * seq_dev, tp_at * wide : (tp_at + 1) * wide] = recv_ref[
            i
        ].astype(F32)
    projected = jnp.dot(rows_ref[...].astype(BF16), weight_ref[...], preferred_element_type=F32)
    after = (own_ref[...].astype(F32) + projected).astype(BF16)
    after_ref[...] = after
    for i in range(out_ref.shape[0]):
        out_ref[i] = after


def feed_kernel(cut, recv_ref, gain_ref, gate_ref, up_ref, down_ref, out_ref, gate_cols, up_cols):
    members, rows, columns = recv_ref.shape
    contract = (((1,), (1,)), ((), ()))
    squares = 0.0
    gain = spread(gain_ref)
    sums = [0.0, 0.0]
    group = 1
    for k in range(members // group):
        pieces = []
        for i in range(k * group, (k + 1) * group):
            piece = recv_ref[i].astype(F32)
            squares = squares + jnp.sum(piece * piece, axis=1, keepdims=True)
            pieces.append((piece * gain[:, i * columns : (i + 1) * columns]).astype(BF16))
        scaled = jnp.concatenate(pieces, axis=1)
        at = slice(k * group * columns, (k + 1) * group * columns)
        for j, (weight, cols) in enumerate(((gate_ref, gate_cols), (up_ref, up_cols))):
            tall = lax.dot_general(weight[:cut, at], scaled, contract, preferred_element_type=F32)
            cols[...] = tall if k == 0 else cols[...] + tall
            sums[j] = sums[j] + lax.dot_general(scaled, weight[cut:, at], contract, preferred_element_type=F32)
    inv = lax.rsqrt(squares / (members * columns) + EPS)
    inv_row = jnp.transpose(jnp.broadcast_to(inv, (rows, LANES)))[:1]
    gate = gate_cols[...] * inv_row
    tall = (gate / (1.0 + jnp.exp(-gate)) * (up_cols[...] * inv_row)).astype(BF16)
    gate = sums[0] * inv
    flat = (gate / (1.0 + jnp.exp(-gate)) * (sums[1] * inv)).astype(BF16)
    for i in range(members):
        at = slice(i * columns, (i + 1) * columns)
        share = lax.dot_general(
            tall, down_ref[:cut, at], (((0,), (0,)), ((), ())), preferred_element_type=F32
        )
        share = share + jnp.dot(flat, down_ref[cut:, at], preferred_element_type=F32)
        out_ref[i] = share.astype(BF16)


def finish_kernel(recv_ref, after_ref, out_ref):
    total = after_ref[...].astype(F32)
    for i in range(recv_ref.shape[0]):
        total = total + recv_ref[i].astype(F32)
    out_ref[...] = total.astype(BF16)


MIB = 1 << 20


def shards(
    tokens,
    lengths,
    state,
    cache_keys,
    cache_values,
    cache_rates,
    attn_gain,
    w_query,
    w_key,
    w_value,
    w_gate,
    w_decay,
    head_gain,
    w_out,
    mlp_gain,
    w_mlp_gate,
    w_mlp_up,
    w_mlp_down,
):
    seq_dev, heads_dev, key_dim, value_dim = state.shape
    width = mlp_gain.shape[0]
    n_kv, n_tp = lax.axis_size("kv"), lax.axis_size("tp")
    members = n_kv * n_tp
    rows, columns = tokens.shape
    other = lax.ppermute(tokens, "tp", [(i, n_tp - 1 - i) for i in range(n_tp)])
    wide = heads_dev * (3 * key_dim + 2 * value_dim) + LANES
    anywhere = pl.BlockSpec(memory_space=pl.ANY)
    weights = (w_query, w_key, w_decay, w_value, w_gate)
    moved = sum(w.size for w in weights) * 2
    parts = call(
        lambda *refs: project_kernel(seq_dev, *refs),
        [jax.ShapeDtypeStruct((seq_dev, wide), F32 if step == 0 else BF16) for step in range(n_kv)],
        [anywhere, vmem_spec()] + [anywhere] * 6,
        [pltpu.VMEM(tokens.shape, BF16), pltpu.VMEM((attn_gain.size // LANES, LANES), BF16)]
        + [pltpu.VMEM(w.shape, BF16) for w in weights]
        + [pltpu.VMEM((rows, wide), F32), pltpu.SemaphoreType.DMA((7,))],
        16 * MIB,
        10**10,
        moved,
        "project",
    )(in_hbm(tokens), other, in_hbm(attn_gain.reshape(-1, LANES)), *(in_hbm(w) for w in weights))
    parts = list(parts)
    own = parts[0]
    for step in range(1, n_kv):
        parts[step] = lax.ppermute(parts[step], "kv", [(i, i ^ step) for i in range(n_kv)])
    moved = state.size * 6 + cache_rates.size * 8
    mixed, total = call(
        gather_kernel,
        [
            jax.ShapeDtypeStruct(state.shape, BF16),
            jax.ShapeDtypeStruct((seq_dev, heads_dev * key_dim), F32),
        ],
        [pl.BlockSpec(memory_space=pltpu.SMEM), anywhere] + [vmem_spec()] * 4,
        [],
        4 * MIB,
        10**9,
        moved,
        "gather",
    )(lengths, own, in_vmem(state), in_vmem(cache_keys), in_vmem(cache_values), in_vmem(cache_rates))
    send = call(
        lambda *refs: attend_kernel(width, refs[:n_kv], *refs[n_kv:]),
        jax.ShapeDtypeStruct((members, seq_dev, heads_dev * value_dim), BF16),
        [vmem_spec()] * (n_kv + 3),
        [pltpu.VMEM((seq_dev, heads_dev * value_dim), F32)],
        4 * MIB,
        4 * 10**10,
        state.size * 2,
        "attend",
    )(own, *parts[:0:-1], mixed, total, in_vmem(head_gain))
    recv = lax.all_to_all(send, ("kv", "tp"), 0, 0, tiled=True)
    send, after = call(
        lambda *refs: output_kernel(n_tp, *refs),
        (jax.ShapeDtypeStruct((members, rows, columns), BF16), jax.ShapeDtypeStruct((rows, columns), BF16)),
        [vmem_spec()] * 3,
        [pltpu.VMEM((rows, w_out.shape[0]), F32)],
        2 * MIB,
        10**6,
        w_out.size * 2,
        "output",
    )(recv, in_vmem(w_out), in_vmem(tokens))
    recv = lax.all_to_all(send, ("kv", "tp"), 0, 0, tiled=True)
    moved = (w_mlp_gate.size + w_mlp_up.size + w_mlp_down.size) * 2
    cut = w_mlp_down.shape[0] // 64 * 16
    send = call(
        lambda *refs: feed_kernel(cut, *refs),
        jax.ShapeDtypeStruct((members, rows, columns), BF16),
        [vmem_spec()] * 5,
        [pltpu.VMEM((cut, rows), F32)] * 2,
        4 * MIB,
        rows * moved,
        moved,
        "feed",
    )(recv, in_vmem(mlp_gain.reshape(-1, LANES)), in_vmem(w_mlp_gate.T), in_vmem(w_mlp_up.T), in_vmem(w_mlp_down))
    recv = lax.all_to_all(send, ("kv", "tp"), 0, 0, tiled=True)
    return call(
        finish_kernel,
        jax.ShapeDtypeStruct((rows, columns), BF16),
        [vmem_spec()] * 2,
        [],
        2 * MIB,
        rows * columns * members,
        rows * columns * members * 2,
        "finish",
    )(recv, after)


def solution(mesh):
    placed = (
        P("dp", ("kv", "tp")),
        P(("dp", "kv")),
        P(("dp", "kv"), "tp", None, None),
        P(("dp", "kv"), "tp", None, None),
        P(("dp", "kv"), "tp", None, None),
        P(("dp", "kv"), "tp", None, None),
        P("kv"),
        P("kv", "tp"),
        P("kv", "tp"),
        P("kv", "tp"),
        P("kv", "tp"),
        P("kv", "tp"),
        P("tp", None),
        P(None, ("kv", "tp")),
        P(),
        P(None, ("kv", "tp")),
        P(None, ("kv", "tp")),
        P(("kv", "tp"), None),
    )
    sizes = mesh.shape

    def body(*args):
        fits = sizes["tp"] == 2 and sizes["kv"] == 4 and args[13].shape[1] % LANES == 0
        return (shards if fits else plain_shards)(*args)

    return jax.shard_map(
        body, mesh=mesh, in_specs=placed, out_specs=P("dp", ("kv", "tp")), check_vma=False
    )
```

```python
import jax
import jax.numpy as jnp
from jax import lax
from jax.experimental import pallas as pl
from jax.experimental.pallas import tpu as pltpu
from jax.sharding import PartitionSpec as P

EPS = 1e-06
GATE_NORM = 16.0
exact_mode = lax.Precision.HIGHEST


def front_part(query, key_new, log_decay, state, cache_keys, cache_rates, lengths):
    span = cache_keys.shape[2]
    live = (jnp.arange(span, dtype=jnp.int32)[None, :] < lengths[:, None]).astype(jnp.float32)
    running = jnp.cumsum(cache_rates * live[:, None, :, None], axis=2)
    total = running[:, :, -1:, :]
    weight = jnp.exp(running - total + log_decay[:, :, None, :])
    scores = (
        jnp.einsum(
            "bhd,bhjd->bhj", query, weight * cache_keys.astype(jnp.float32), precision=exact_mode
        )
        * live[:, None, :]
    )
    carried = jnp.einsum(
        "bhd,bhde->bhe", query * jnp.exp(log_decay - total[:, :, 0, :]), state, precision=exact_mode
    )
    own = jnp.sum(query * key_new, axis=-1, keepdims=True)
    return (scores, carried, own)


def back_part(scores, carried, own, value_new, cache_values, gate, head_gain):
    inner = jnp.einsum(
        "bhj,bhje->bhe", scores, cache_values.astype(jnp.float32), precision=exact_mode
    )
    attended = carried + inner + own * value_new
    normed = attended * lax.rsqrt(jnp.mean(attended * attended, axis=-1, keepdims=True) + EPS)
    normed = normed * head_gain.astype(jnp.float32)
    return (jax.nn.silu(gate) * normed).astype(jnp.bfloat16)


def open_heads(
    query_sum, key_sum, decay_sum, own_squares, width, state, cache_keys, cache_rates, lengths
):
    seq_dev, heads_dev, key_dim = (state.shape[0], state.shape[1], state.shape[2])
    inv_rms = lax.rsqrt(own_squares / width + EPS)[:, None]
    query = (query_sum * inv_rms * key_dim ** (-0.5)).reshape(seq_dev, heads_dev, key_dim)
    key_new = (key_sum * inv_rms).reshape(seq_dev, heads_dev, key_dim)
    log_decay = (jax.nn.log_sigmoid(decay_sum * inv_rms) / GATE_NORM).reshape(
        seq_dev, heads_dev, key_dim
    )
    scores, carried, own = front_part(
        query, key_new, log_decay, state, cache_keys, cache_rates, lengths
    )
    return (inv_rms, scores, carried, own)


def close_heads(opened, value_sum, gate_sum, cache_values, head_gain):
    inv_rms, scores, carried, own = opened
    seq_dev, heads_dev, value_dim = carried.shape
    value_new = (value_sum * inv_rms).reshape(seq_dev, heads_dev, value_dim)
    gate = (gate_sum * inv_rms).reshape(seq_dev, heads_dev, value_dim)
    heads = back_part(scores, carried, own, value_new, cache_values, gate, head_gain)
    return heads.reshape(seq_dev, heads_dev * value_dim)


def plain_shards(
    tokens,
    lengths,
    state,
    cache_keys,
    cache_values,
    cache_rates,
    attn_gain,
    w_query,
    w_key,
    w_value,
    w_gate,
    w_decay,
    head_gain,
    w_out,
    mlp_gain,
    w_mlp_gate,
    w_mlp_up,
    w_mlp_down,
):
    seq_dev, heads_dev, value_dim = (state.shape[0], state.shape[1], state.shape[3])
    width = mlp_gain.shape[0]
    n_kv = lax.axis_size("kv")
    n_tp = lax.axis_size("tp")
    block = lax.all_gather(tokens, "tp", axis=1, tiled=True).astype(jnp.float32)
    squares = jnp.sum(block * block, axis=1)
    scaled = (block * attn_gain.astype(jnp.float32)).astype(jnp.bfloat16)
    query_part = jnp.dot(scaled, w_query, preferred_element_type=jnp.float32)
    key_part = jnp.dot(scaled, w_key, preferred_element_type=jnp.float32)
    decay_part = jnp.dot(scaled, w_decay, preferred_element_type=jnp.float32)
    value_part = jnp.dot(scaled, w_value, preferred_element_type=jnp.float32)
    gate_part = jnp.dot(scaled, w_gate, preferred_element_type=jnp.float32)
    every_square = lax.psum(squares, "kv")
    own_squares = lax.dynamic_slice_in_dim(every_square, lax.axis_index("kv") * seq_dev, seq_dev)
    query_sum, key_sum, decay_sum, value_sum, gate_sum = (
        lax.psum_scatter(query_part, "kv", scatter_dimension=0, tiled=True),
        lax.psum_scatter(key_part, "kv", scatter_dimension=0, tiled=True),
        lax.psum_scatter(decay_part, "kv", scatter_dimension=0, tiled=True),
        lax.psum_scatter(value_part, "kv", scatter_dimension=0, tiled=True),
        lax.psum_scatter(gate_part, "kv", scatter_dimension=0, tiled=True),
    )
    opened = open_heads(
        query_sum, key_sum, decay_sum, own_squares, width, state, cache_keys, cache_rates, lengths
    )
    heads = close_heads(opened, value_sum, gate_sum, cache_values, head_gain)
    columns = w_out.shape[1]
    stacked = w_out.reshape(n_tp, heads_dev * value_dim, columns)
    piece = lax.all_gather(
        heads.reshape(1, seq_dev, heads_dev * value_dim), ("kv", "tp"), axis=0, tiled=True
    )
    terms = jnp.einsum("psk,tkc->ptsc", piece, stacked, preferred_element_type=jnp.float32)
    owner = jnp.arange(piece.shape[0], dtype=jnp.int32)
    row_match = (owner // n_tp)[:, None, None] == jnp.arange(n_kv, dtype=jnp.int32)[None, :, None]
    head_match = (owner % n_tp)[:, None, None] == jnp.arange(n_tp, dtype=jnp.int32)[None, None, :]
    chosen = (row_match & head_match).astype(jnp.float32)
    projected = jnp.einsum("prt,ptsc->rsc", chosen, terms, precision=exact_mode)
    projected = projected.reshape(n_kv * seq_dev, columns)
    after = (tokens.astype(jnp.float32) + projected).astype(jnp.bfloat16)
    whole = lax.all_gather(after, ("kv", "tp"), axis=1, tiled=True).astype(jnp.float32)
    inv_second = lax.rsqrt(jnp.mean(whole * whole, axis=1, keepdims=True) + EPS)
    normed = (whole * inv_second * mlp_gain.astype(jnp.float32)).astype(jnp.bfloat16)
    gate_ff = jnp.dot(normed, w_mlp_gate, preferred_element_type=jnp.float32)
    up_ff = jnp.dot(normed, w_mlp_up, preferred_element_type=jnp.float32)
    hidden = (jax.nn.silu(gate_ff) * up_ff).astype(jnp.bfloat16)
    terms = jnp.dot(hidden, w_mlp_down, preferred_element_type=jnp.float32)
    own_share = lax.psum_scatter(terms, ("kv", "tp"), scatter_dimension=1, tiled=True)
    return (after.astype(jnp.float32) + own_share).astype(jnp.bfloat16)


F32 = jnp.float32
BF16 = jnp.bfloat16
LANES = 128


def in_vmem(array):
    return pltpu.with_memory_space_constraint(array, pltpu.VMEM)


def in_hbm(array):
    return pltpu.with_memory_space_constraint(array, pltpu.HBM)


def vmem_spec():
    return pl.BlockSpec(memory_space=pltpu.VMEM)


def call(kernel, out_shape, in_specs, scratch, limit, flops, moved, name):
    return pl.pallas_call(
        kernel,
        out_shape=out_shape,
        in_specs=in_specs,
        out_specs=jax.tree.map(lambda _: vmem_spec(), out_shape),
        scratch_shapes=scratch,
        compiler_params=pltpu.CompilerParams(vmem_limit_bytes=limit),
        cost_estimate=pl.CostEstimate(flops=flops, bytes_accessed=moved, transcendentals=0),
        name=name,
    )


def spread(gain_ref):
    rows = gain_ref[...].astype(F32)
    return jnp.concatenate([rows[i : i + 1] for i in range(rows.shape[0])], axis=1)


def by_partner(block, seq_dev, n_kv):
    me = lax.axis_index("kv")
    place = lax.broadcasted_iota(jnp.int32, block.shape, 0) // seq_dev
    rows = block.shape[0]
    bit = 1
    while bit < n_kv:
        down = pltpu.roll(block, bit * seq_dev, 0)
        up = pltpu.roll(block, rows - bit * seq_dev, 0)
        swapped = jnp.where((place & bit) == 0, up, down)
        block = jnp.where((me & bit) == 0, block, swapped)
        bit *= 2
    return block


def project_kernel(
    seq_dev, own_hbm, other_ref, gain_hbm, wq, wk, wd, wv, wg, *rest
):
    out_refs, (own_ref, gain_ref, bq, bk, bd, bv, bg, acc, sems) = rest[:-9], rest[-9:]
    pairs = ((own_hbm, own_ref), (gain_hbm, gain_ref), (wq, bq), (wk, bk), (wd, bd), (wv, bv), (wg, bg))
    copies = [pltpu.make_async_copy(src, dst, sems.at[i]) for i, (src, dst) in enumerate(pairs)]
    for copy in copies:
        copy.start()
    copies[0].wait()
    copies[1].wait()
    own = own_ref[...].astype(F32)
    other = other_ref[...].astype(F32)
    first = lax.axis_index("tp") == 0
    low = jnp.where(first, own, other)
    high = jnp.where(first, other, own)
    block = by_partner(jnp.concatenate([low, high], axis=1), seq_dev, len(out_refs))
    total = jnp.sum(block * block, axis=1, keepdims=True)
    scaled = (block * spread(gain_ref)).astype(BF16)
    at = 0
    for copy, (_, buf) in zip(copies[2:], pairs[2:]):
        copy.wait()
        acc[:, at : at + buf.shape[1]] = jnp.dot(scaled, buf[...], preferred_element_type=F32)
        at += buf.shape[1]
    lane = lax.broadcasted_iota(jnp.int32, (block.shape[0], LANES), 1)
    upper = total.astype(BF16).astype(F32)
    lower = total - upper
    acc[:, at : at + LANES] = jnp.where(lane == 0, upper, jnp.where(lane == 1, lower, 0.0))
    for step, out_ref in enumerate(out_refs):
        out_ref[...] = acc[step * seq_dev : (step + 1) * seq_dev, :].astype(out_ref.dtype)


def split_rows(row):
    upper = row.astype(BF16).astype(F32)
    lower = row - upper
    shape = (8, row.shape[1])
    at = lax.broadcasted_iota(jnp.int32, shape, 0)
    upper = jnp.broadcast_to(upper, shape)
    lower = jnp.broadcast_to(lower, shape)
    return jnp.where(at == 0, upper, jnp.where(at == 1, lower, 0.0)).astype(BF16)


def gather_kernel(
    lengths_ref, _, state_ref, keys_ref, values_ref, rates_ref, gain_ref, mixed_ref, total_ref, own_gain_ref
):
    seq_dev, heads_dev, key_dim, value_dim = state_ref.shape
    span = keys_ref.shape[2]
    row_at = lax.broadcasted_iota(jnp.int32, (span, span), 0)
    col_at = lax.broadcasted_iota(jnp.int32, (span, span), 1)
    upto = jnp.where(col_at <= row_at, 1.0, 0.0).astype(BF16)
    slot = lax.broadcasted_iota(jnp.int32, (span, 1), 0)
    gain = spread(gain_ref)
    columns = own_gain_ref.shape[1]
    member = lax.axis_index("kv") * lax.axis_size("tp") + lax.axis_index("tp")
    own_gain = gain[:, :columns]
    for i in range(1, gain.shape[1] // columns):
        own_gain = jnp.where(member == i, gain[:, i * columns : (i + 1) * columns], own_gain)
    own_gain_ref[...] = own_gain
    for s in range(seq_dev):
        live = (slot < lengths_ref[s]).astype(F32)
        for h in range(heads_dev):
            rates = rates_ref[s, h] * live
            upper = rates.astype(BF16)
            lower = (rates - upper.astype(F32)).astype(BF16)
            running = jnp.dot(upto, upper, preferred_element_type=F32)
            running = running + jnp.dot(upto, lower, preferred_element_type=F32)
            total_ref[s : s + 1, h * key_dim : (h + 1) * key_dim] = running[span - 1 :]
            grown = (jnp.exp(running) * keys_ref[s, h].astype(F32) * live).astype(BF16)
            added = lax.dot_general(
                grown, values_ref[s, h], (((0,), (0,)), ((), ())), preferred_element_type=F32
            )
            mixed_ref[s, h] = (state_ref[s, h] + added).astype(BF16)


def attend_kernel(width, parts, mixed_ref, total_ref, gain_ref, out_ref, heads_ref):
    seq_dev, heads_dev, key_dim, value_dim = mixed_ref.shape
    got = parts[0][...]
    for part in parts[1:]:
        got = got + part[...].astype(F32)
    keys_all, values_all = heads_dev * key_dim, heads_dev * value_dim
    ends = [0, keys_all, 2 * keys_all, 3 * keys_all]
    ends += [ends[3] + values_all, ends[3] + 2 * values_all]
    squares = jnp.sum(got[:, ends[5] :], axis=1, keepdims=True)
    inv_rms = lax.rsqrt(squares / width + EPS)
    query = got[:, ends[0] : ends[1]] * inv_rms * key_dim ** (-0.5)
    key_new = got[:, ends[1] : ends[2]] * inv_rms
    raw = got[:, ends[2] : ends[3]] * inv_rms
    log_decay = (jnp.minimum(raw, 0.0) - jnp.log(1.0 + jnp.exp(-jnp.abs(raw)))) / GATE_NORM
    value_new = got[:, ends[3] : ends[4]] * inv_rms
    gate = got[:, ends[4] : ends[5]] * inv_rms
    gate = gate / (1.0 + jnp.exp(-gate))
    decayed = query * jnp.exp(log_decay - total_ref[...])
    product = query * key_new
    for s in range(seq_dev):
        for h in range(heads_dev):
            ks, vs = slice(h * key_dim, (h + 1) * key_dim), slice(h * value_dim, (h + 1) * value_dim)
            rows = split_rows(decayed[s : s + 1, ks])
            mixed = jnp.dot(rows, mixed_ref[s, h], preferred_element_type=F32)
            own = jnp.sum(product[s : s + 1, ks], axis=1, keepdims=True)
            heads_ref[s : s + 1, vs] = jnp.sum(mixed, axis=0, keepdims=True) + own * value_new[s : s + 1, vs]
    pieces = []
    for h in range(heads_dev):
        vs = slice(h * value_dim, (h + 1) * value_dim)
        attended = heads_ref[:, vs]
        scale = lax.rsqrt(jnp.mean(attended * attended, axis=1, keepdims=True) + EPS)
        pieces.append(gate[:, vs] * (attended * scale * gain_ref[h : h + 1, :].astype(F32)))
    heads = jnp.concatenate(pieces, axis=1).astype(BF16)
    for i in range(out_ref.shape[0]):
        out_ref[i] = heads


def output_kernel(n_tp, recv_ref, weight_ref, own_ref, gain_ref, after_ref, scaled_ref, rows_ref):
    seq_dev, wide = recv_ref.shape[1], recv_ref.shape[2]
    for i in range(recv_ref.shape[0]):
        kv_at, tp_at = divmod(i, n_tp)
        rows_ref[kv_at * seq_dev : (kv_at + 1) * seq_dev, tp_at * wide : (tp_at + 1) * wide] = recv_ref[
            i
        ].astype(F32)
    projected = jnp.dot(rows_ref[...].astype(BF16), weight_ref[...], preferred_element_type=F32)
    after = (own_ref[...].astype(F32) + projected).astype(BF16)
    after_ref[...] = after
    after = after.astype(F32)
    columns = after.shape[1]
    scaled_ref[:, :columns] = (after * gain_ref[...]).astype(BF16)
    squares = jnp.sum(after * after, axis=1, keepdims=True)
    lane = lax.broadcasted_iota(jnp.int32, (after.shape[0], LANES), 1)
    upper = squares.astype(BF16).astype(F32)
    lower = squares - upper
    scaled_ref[:, columns:] = jnp.where(lane == 0, upper, jnp.where(lane == 1, lower, 0.0)).astype(BF16)


def member_columns(step, other, columns):
    tp = lax.axis_index("tp")
    tp = 1 - tp if other else tp
    member = (lax.axis_index("kv") ^ step) * lax.axis_size("tp") + tp
    return pl.ds(pl.multiple_of(member * columns, columns), columns)


def grow(cut, columns, pieces, gate_ref, up_ref, tall_refs, flats, squares, fresh):
    contract = (((1,), (1,)), ((), ()))
    for piece, step, other in pieces:
        at = member_columns(step, other, columns)
        rows = piece[:, :columns]
        squares = squares + jnp.sum(piece[:, columns:].astype(F32), axis=1, keepdims=True)
        for j, weight in enumerate((gate_ref, up_ref)):
            tall = lax.dot_general(weight[:cut, at], rows, contract, preferred_element_type=F32)
            tall_refs[j][...] = tall if fresh else tall_refs[j][...] + tall
            flats[j] = flats[j] + lax.dot_general(rows, weight[cut:, at], contract, preferred_element_type=F32)
        fresh = False
    return squares


def first_kernel(cut, columns, own_ref, other_ref, gate_ref, up_ref, _, *sums):
    talls, flat_refs, squares_ref = sums[:2], sums[2:4], sums[4]
    flats = [0.0, 0.0]
    pieces = ((own_ref, 0, False), (other_ref, 0, True))
    squares = grow(cut, columns, pieces, gate_ref, up_ref, talls, flats, 0.0, True)
    for ref, flat in zip(flat_refs, flats):
        ref[...] = flat
    squares_ref[...] = jnp.broadcast_to(squares, squares_ref.shape)


def next_sums(cut, columns, count, other, refs, talls):
    pieces = [(refs[i], i + 1, other) for i in range(count)]
    gate_ref, up_ref = refs[count : count + 2]
    old_talls, flat_refs, squares_ref = refs[count + 2 : count + 4], refs[count + 4 : count + 6], refs[count + 6]
    for new, old in zip(talls, old_talls):
        new[...] = old[...]
    flats = [ref[...] for ref in flat_refs]
    squares = grow(cut, columns, pieces, gate_ref, up_ref, talls, flats, squares_ref[:, :1], False)
    return flats, squares


def second_kernel(cut, columns, count, *refs):
    sums = refs[count + 8 :]
    flats, squares = next_sums(cut, columns, count, False, refs, sums[:2])
    for ref, flat in zip(sums[2:4], flats):
        ref[...] = flat
    sums[4][...] = jnp.broadcast_to(squares, sums[4].shape)


def shares(cut, columns, other, tall, flat, down_ref, out_refs):
    for step, out_ref in enumerate(out_refs):
        at = member_columns(step, other, columns)
        share = lax.dot_general(
            tall, down_ref[:cut, at], (((0,), (0,)), ((), ())), preferred_element_type=F32
        )
        share = share + jnp.dot(flat, down_ref[cut:, at], preferred_element_type=F32)
        out_ref[...] = share.astype(out_ref.dtype)


def third_kernel(cut, columns, count, width, *refs):
    down_ref, (send_ref, tall_ref, flat_ref), talls = refs[count + 7], refs[count + 8 : -2], refs[-2:]
    flats, squares = next_sums(cut, columns, count, True, refs, talls)
    inv = lax.rsqrt(squares / width + EPS)
    rows = inv.shape[0]
    inv_row = jnp.transpose(jnp.broadcast_to(inv, (rows, LANES)))[:1]
    gate = talls[0][...] * inv_row
    tall = (gate / (1.0 + jnp.exp(-gate)) * (talls[1][...] * inv_row)).astype(BF16)
    gate = flats[0] * inv
    flat = (gate / (1.0 + jnp.exp(-gate)) * (flats[1] * inv)).astype(BF16)
    tall_ref[...] = tall
    flat_ref[...] = flat
    outs = [send_ref.at[:, i * columns : (i + 1) * columns] for i in range(count + 1)]
    shares(cut, columns, True, tall, flat, down_ref, outs)


def fourth_kernel(cut, columns, tall_ref, flat_ref, down_ref, out_ref):
    outs = [out_ref.at[:, i * columns : (i + 1) * columns] for i in range(out_ref.shape[1] // columns)]
    shares(cut, columns, False, tall_ref[...], flat_ref[...], down_ref, outs)


def merge_kernel(columns, own_ref, recv_ref, after_ref, *out_refs):
    for step, out_ref in enumerate(out_refs):
        at = slice(step * columns, (step + 1) * columns)
        total = own_ref[:, at] + recv_ref[:, at].astype(F32)
        if step == 0:
            total = total + after_ref[...].astype(F32)
        out_ref[...] = total.astype(out_ref.dtype)


def finish_kernel(*refs):
    total = refs[0][...]
    for part in refs[1:-1]:
        total = total + part[...].astype(F32)
    refs[-1][...] = total.astype(BF16)


MIB = 1 << 20


def shards(
    tokens,
    lengths,
    state,
    cache_keys,
    cache_values,
    cache_rates,
    attn_gain,
    w_query,
    w_key,
    w_value,
    w_gate,
    w_decay,
    head_gain,
    w_out,
    mlp_gain,
    w_mlp_gate,
    w_mlp_up,
    w_mlp_down,
):
    seq_dev, heads_dev, key_dim, value_dim = state.shape
    width = mlp_gain.shape[0]
    n_kv, n_tp = lax.axis_size("kv"), lax.axis_size("tp")
    members = n_kv * n_tp
    rows, columns = tokens.shape
    other = lax.ppermute(tokens, "tp", [(i, n_tp - 1 - i) for i in range(n_tp)])
    wide = heads_dev * (3 * key_dim + 2 * value_dim) + LANES
    anywhere = pl.BlockSpec(memory_space=pl.ANY)
    weights = (w_query, w_key, w_decay, w_value, w_gate)
    moved = sum(w.size for w in weights) * 2
    parts = call(
        lambda *refs: project_kernel(seq_dev, *refs),
        [jax.ShapeDtypeStruct((seq_dev, wide), F32 if step == 0 else BF16) for step in range(n_kv)],
        [anywhere, vmem_spec()] + [anywhere] * 6,
        [pltpu.VMEM(tokens.shape, BF16), pltpu.VMEM((attn_gain.size // LANES, LANES), BF16)]
        + [pltpu.VMEM(w.shape, BF16) for w in weights]
        + [pltpu.VMEM((rows, wide), F32), pltpu.SemaphoreType.DMA((7,))],
        16 * MIB,
        10**10,
        moved,
        "project",
    )(in_hbm(tokens), other, in_hbm(attn_gain.reshape(-1, LANES)), *(in_hbm(w) for w in weights))
    parts = list(parts)
    own = parts[0]
    for step in range(1, n_kv):
        parts[step] = lax.ppermute(parts[step], "kv", [(i, i ^ step) for i in range(n_kv)])
    moved = state.size * 6 + cache_rates.size * 8
    mixed, total, own_gain = call(
        gather_kernel,
        [
            jax.ShapeDtypeStruct(state.shape, BF16),
            jax.ShapeDtypeStruct((seq_dev, heads_dev * key_dim), F32),
            jax.ShapeDtypeStruct((1, columns), F32),
        ],
        [pl.BlockSpec(memory_space=pltpu.SMEM), anywhere] + [vmem_spec()] * 5,
        [],
        4 * MIB,
        4 * 10**10,
        moved,
        "gather",
    )(lengths, own, in_vmem(state), in_vmem(cache_keys), in_vmem(cache_values), in_vmem(cache_rates), in_vmem(mlp_gain.reshape(-1, LANES)))
    send = call(
        lambda *refs: attend_kernel(width, refs[:n_kv], *refs[n_kv:]),
        jax.ShapeDtypeStruct((members, seq_dev, heads_dev * value_dim), BF16),
        [vmem_spec()] * (n_kv + 3),
        [pltpu.VMEM((seq_dev, heads_dev * value_dim), F32)],
        4 * MIB,
        10**6,
        state.size * 2,
        "attend",
    )(own, *parts[:0:-1], mixed, total, in_vmem(head_gain))
    recv = lax.all_to_all(send, ("kv", "tp"), 0, 0, tiled=True)
    narrow = jax.ShapeDtypeStruct((rows, columns + LANES), BF16)
    after, scaled = call(
        lambda *refs: output_kernel(n_tp, *refs),
        (jax.ShapeDtypeStruct((rows, columns), BF16), narrow),
        [vmem_spec()] * 4,
        [pltpu.VMEM((rows, w_out.shape[0]), F32)],
        2 * MIB,
        10**6,
        w_out.size * 2,
        "output",
    )(recv, in_vmem(w_out), in_vmem(tokens), own_gain)
    swap = [(i, n_tp - 1 - i) for i in range(n_tp)]
    far = n_kv - 1
    got = [lax.ppermute(scaled, "kv", [(i, i ^ step) for i in range(n_kv)]) for step in range(1, n_kv)]
    beside = lax.ppermute(scaled, "tp", swap)
    hidden = w_mlp_down.shape[0]
    cut = w_mlp_down.shape[0] // 64 * 16
    sums = (
        [jax.ShapeDtypeStruct((cut, rows), F32)] * 2
        + [jax.ShapeDtypeStruct((rows, hidden - cut), F32)] * 2
        + [jax.ShapeDtypeStruct((rows, LANES), F32)]
    )
    down = in_vmem(w_mlp_down)
    gate_up = (in_vmem(w_mlp_gate.T), in_vmem(w_mlp_up.T))
    running = call(
        lambda *refs: first_kernel(cut, columns, *refs),
        sums,
        [vmem_spec()] * 5,
        [],
        4 * MIB,
        MIB,
        MIB,
        "feed_first",
    )(scaled, beside, *gate_up, down)
    got, running = lax.optimization_barrier((got, running))
    beside = [lax.ppermute(piece, "tp", swap) for piece in got]
    running = call(
        lambda *refs: second_kernel(cut, columns, far, *refs),
        sums,
        [vmem_spec()] * (far + 8),
        [],
        4 * MIB,
        MIB,
        MIB,
        "feed_second",
    )(*got, *gate_up, *running, down)
    send, tall, flat = call(
        lambda *refs: third_kernel(cut, columns, far, width, *refs),
        [
            jax.ShapeDtypeStruct((rows, n_kv * columns), BF16),
            jax.ShapeDtypeStruct((cut, rows), BF16),
            jax.ShapeDtypeStruct((rows, hidden - cut), BF16),
        ],
        [vmem_spec()] * (far + 8),
        [pltpu.VMEM((cut, rows), F32)] * 2,
        4 * MIB,
        MIB,
        MIB,
        "feed_third",
    )(*beside, *gate_up, *running, down)
    recv = lax.ppermute(send, "tp", swap)
    own = call(
        lambda *refs: fourth_kernel(cut, columns, *refs),
        jax.ShapeDtypeStruct((rows, n_kv * columns), F32),
        [vmem_spec()] * 3,
        [],
        4 * MIB,
        MIB,
        MIB,
        "feed_fourth",
    )(tall, flat, down)
    merged = call(
        lambda *refs: merge_kernel(columns, *refs),
        [jax.ShapeDtypeStruct((rows, columns), F32 if step == 0 else BF16) for step in range(n_kv)],
        [vmem_spec()] * 3,
        [],
        2 * MIB,
        rows * columns * n_kv,
        rows * columns * n_kv * 6,
        "merge",
    )(own, recv, after)
    parts = [
        lax.ppermute(merged[step], "kv", [(i, i ^ step) for i in range(n_kv)]) for step in range(1, n_kv)
    ]
    return call(
        finish_kernel,
        jax.ShapeDtypeStruct((rows, columns), BF16),
        [vmem_spec()] * n_kv,
        [],
        2 * MIB,
        rows * columns * n_kv,
        rows * columns * n_kv * 2,
        "finish",
    )(merged[0], *parts[::-1])


def solution(mesh):
    placed = (
        P("dp", ("kv", "tp")),
        P(("dp", "kv")),
        P(("dp", "kv"), "tp", None, None),
        P(("dp", "kv"), "tp", None, None),
        P(("dp", "kv"), "tp", None, None),
        P(("dp", "kv"), "tp", None, None),
        P("kv"),
        P("kv", "tp"),
        P("kv", "tp"),
        P("kv", "tp"),
        P("kv", "tp"),
        P("kv", "tp"),
        P("tp", None),
        P(None, ("kv", "tp")),
        P(),
        P(None, ("kv", "tp")),
        P(None, ("kv", "tp")),
        P(("kv", "tp"), None),
    )
    sizes = mesh.shape

    def body(*args):
        fits = sizes["tp"] == 2 and sizes["kv"] == 4 and args[13].shape[1] % LANES == 0
        return (shards if fits else plain_shards)(*args)

    return jax.shard_map(
        body, mesh=mesh, in_specs=placed, out_specs=P("dp", ("kv", "tp")), check_vma=False
    )
```

```python
import jax
import jax.numpy as jnp
from jax import lax
from jax.experimental import pallas as pl
from jax.experimental.pallas import tpu as pltpu
from jax.sharding import PartitionSpec as P

EPS = 1e-06
GATE_NORM = 16.0
exact_mode = lax.Precision.HIGHEST


def front_part(query, key_new, log_decay, state, cache_keys, cache_rates, lengths):
    span = cache_keys.shape[2]
    live = (jnp.arange(span, dtype=jnp.int32)[None, :] < lengths[:, None]).astype(jnp.float32)
    running = jnp.cumsum(cache_rates * live[:, None, :, None], axis=2)
    total = running[:, :, -1:, :]
    weight = jnp.exp(running - total + log_decay[:, :, None, :])
    scores = (
        jnp.einsum(
            "bhd,bhjd->bhj", query, weight * cache_keys.astype(jnp.float32), precision=exact_mode
        )
        * live[:, None, :]
    )
    carried = jnp.einsum(
        "bhd,bhde->bhe", query * jnp.exp(log_decay - total[:, :, 0, :]), state, precision=exact_mode
    )
    own = jnp.sum(query * key_new, axis=-1, keepdims=True)
    return (scores, carried, own)


def back_part(scores, carried, own, value_new, cache_values, gate, head_gain):
    inner = jnp.einsum(
        "bhj,bhje->bhe", scores, cache_values.astype(jnp.float32), precision=exact_mode
    )
    attended = carried + inner + own * value_new
    normed = attended * lax.rsqrt(jnp.mean(attended * attended, axis=-1, keepdims=True) + EPS)
    normed = normed * head_gain.astype(jnp.float32)
    return (jax.nn.silu(gate) * normed).astype(jnp.bfloat16)


def open_heads(
    query_sum, key_sum, decay_sum, own_squares, width, state, cache_keys, cache_rates, lengths
):
    seq_dev, heads_dev, key_dim = (state.shape[0], state.shape[1], state.shape[2])
    inv_rms = lax.rsqrt(own_squares / width + EPS)[:, None]
    query = (query_sum * inv_rms * key_dim ** (-0.5)).reshape(seq_dev, heads_dev, key_dim)
    key_new = (key_sum * inv_rms).reshape(seq_dev, heads_dev, key_dim)
    log_decay = (jax.nn.log_sigmoid(decay_sum * inv_rms) / GATE_NORM).reshape(
        seq_dev, heads_dev, key_dim
    )
    scores, carried, own = front_part(
        query, key_new, log_decay, state, cache_keys, cache_rates, lengths
    )
    return (inv_rms, scores, carried, own)


def close_heads(opened, value_sum, gate_sum, cache_values, head_gain):
    inv_rms, scores, carried, own = opened
    seq_dev, heads_dev, value_dim = carried.shape
    value_new = (value_sum * inv_rms).reshape(seq_dev, heads_dev, value_dim)
    gate = (gate_sum * inv_rms).reshape(seq_dev, heads_dev, value_dim)
    heads = back_part(scores, carried, own, value_new, cache_values, gate, head_gain)
    return heads.reshape(seq_dev, heads_dev * value_dim)


def plain_shards(
    tokens,
    lengths,
    state,
    cache_keys,
    cache_values,
    cache_rates,
    attn_gain,
    w_query,
    w_key,
    w_value,
    w_gate,
    w_decay,
    head_gain,
    w_out,
    mlp_gain,
    w_mlp_gate,
    w_mlp_up,
    w_mlp_down,
):
    seq_dev, heads_dev, value_dim = (state.shape[0], state.shape[1], state.shape[3])
    width = mlp_gain.shape[0]
    n_kv = lax.axis_size("kv")
    n_tp = lax.axis_size("tp")
    block = lax.all_gather(tokens, "tp", axis=1, tiled=True).astype(jnp.float32)
    squares = jnp.sum(block * block, axis=1)
    scaled = (block * attn_gain.astype(jnp.float32)).astype(jnp.bfloat16)
    query_part = jnp.dot(scaled, w_query, preferred_element_type=jnp.float32)
    key_part = jnp.dot(scaled, w_key, preferred_element_type=jnp.float32)
    decay_part = jnp.dot(scaled, w_decay, preferred_element_type=jnp.float32)
    value_part = jnp.dot(scaled, w_value, preferred_element_type=jnp.float32)
    gate_part = jnp.dot(scaled, w_gate, preferred_element_type=jnp.float32)
    every_square = lax.psum(squares, "kv")
    own_squares = lax.dynamic_slice_in_dim(every_square, lax.axis_index("kv") * seq_dev, seq_dev)
    query_sum, key_sum, decay_sum, value_sum, gate_sum = (
        lax.psum_scatter(query_part, "kv", scatter_dimension=0, tiled=True),
        lax.psum_scatter(key_part, "kv", scatter_dimension=0, tiled=True),
        lax.psum_scatter(decay_part, "kv", scatter_dimension=0, tiled=True),
        lax.psum_scatter(value_part, "kv", scatter_dimension=0, tiled=True),
        lax.psum_scatter(gate_part, "kv", scatter_dimension=0, tiled=True),
    )
    opened = open_heads(
        query_sum, key_sum, decay_sum, own_squares, width, state, cache_keys, cache_rates, lengths
    )
    heads = close_heads(opened, value_sum, gate_sum, cache_values, head_gain)
    columns = w_out.shape[1]
    stacked = w_out.reshape(n_tp, heads_dev * value_dim, columns)
    piece = lax.all_gather(
        heads.reshape(1, seq_dev, heads_dev * value_dim), ("kv", "tp"), axis=0, tiled=True
    )
    terms = jnp.einsum("psk,tkc->ptsc", piece, stacked, preferred_element_type=jnp.float32)
    owner = jnp.arange(piece.shape[0], dtype=jnp.int32)
    row_match = (owner // n_tp)[:, None, None] == jnp.arange(n_kv, dtype=jnp.int32)[None, :, None]
    head_match = (owner % n_tp)[:, None, None] == jnp.arange(n_tp, dtype=jnp.int32)[None, None, :]
    chosen = (row_match & head_match).astype(jnp.float32)
    projected = jnp.einsum("prt,ptsc->rsc", chosen, terms, precision=exact_mode)
    projected = projected.reshape(n_kv * seq_dev, columns)
    after = (tokens.astype(jnp.float32) + projected).astype(jnp.bfloat16)
    whole = lax.all_gather(after, ("kv", "tp"), axis=1, tiled=True).astype(jnp.float32)
    inv_second = lax.rsqrt(jnp.mean(whole * whole, axis=1, keepdims=True) + EPS)
    normed = (whole * inv_second * mlp_gain.astype(jnp.float32)).astype(jnp.bfloat16)
    gate_ff = jnp.dot(normed, w_mlp_gate, preferred_element_type=jnp.float32)
    up_ff = jnp.dot(normed, w_mlp_up, preferred_element_type=jnp.float32)
    hidden = (jax.nn.silu(gate_ff) * up_ff).astype(jnp.bfloat16)
    terms = jnp.dot(hidden, w_mlp_down, preferred_element_type=jnp.float32)
    own_share = lax.psum_scatter(terms, ("kv", "tp"), scatter_dimension=1, tiled=True)
    return (after.astype(jnp.float32) + own_share).astype(jnp.bfloat16)


F32 = jnp.float32
BF16 = jnp.bfloat16
LANES = 128


def in_vmem(array):
    return pltpu.with_memory_space_constraint(array, pltpu.VMEM)


def in_hbm(array):
    return pltpu.with_memory_space_constraint(array, pltpu.HBM)


def vmem_spec():
    return pl.BlockSpec(memory_space=pltpu.VMEM)


def call(kernel, out_shape, in_specs, scratch, limit, flops, moved, name):
    return pl.pallas_call(
        kernel,
        out_shape=out_shape,
        in_specs=in_specs,
        out_specs=jax.tree.map(lambda _: vmem_spec(), out_shape),
        scratch_shapes=scratch,
        compiler_params=pltpu.CompilerParams(vmem_limit_bytes=limit),
        cost_estimate=pl.CostEstimate(flops=flops, bytes_accessed=moved, transcendentals=0),
        name=name,
    )


def spread(gain_ref):
    rows = gain_ref[...].astype(F32)
    return jnp.concatenate([rows[i : i + 1] for i in range(rows.shape[0])], axis=1)


def by_partner(block, seq_dev, n_kv):
    me = lax.axis_index("kv")
    place = lax.broadcasted_iota(jnp.int32, block.shape, 0) // seq_dev
    rows = block.shape[0]
    bit = 1
    while bit < n_kv:
        down = pltpu.roll(block, bit * seq_dev, 0)
        up = pltpu.roll(block, rows - bit * seq_dev, 0)
        swapped = jnp.where((place & bit) == 0, up, down)
        block = jnp.where((me & bit) == 0, block, swapped)
        bit *= 2
    return block


def project_kernel(
    seq_dev, own_hbm, other_ref, gain_hbm, wq, wk, wd, wv, wg, *rest
):
    out_refs, (own_ref, gain_ref, bq, bk, bd, bv, bg, acc, sems) = rest[:-9], rest[-9:]
    pairs = ((own_hbm, own_ref), (gain_hbm, gain_ref), (wq, bq), (wk, bk), (wd, bd), (wv, bv), (wg, bg))
    copies = [pltpu.make_async_copy(src, dst, sems.at[i]) for i, (src, dst) in enumerate(pairs)]
    for copy in copies:
        copy.start()
    copies[0].wait()
    copies[1].wait()
    own = own_ref[...].astype(F32)
    other = other_ref[...].astype(F32)
    first = lax.axis_index("tp") == 0
    low = jnp.where(first, own, other)
    high = jnp.where(first, other, own)
    block = by_partner(jnp.concatenate([low, high], axis=1), seq_dev, len(out_refs))
    total = jnp.sum(block * block, axis=1, keepdims=True)
    scaled = (block * spread(gain_ref)).astype(BF16)
    at = 0
    for copy, (_, buf) in zip(copies[2:], pairs[2:]):
        copy.wait()
        acc[:, at : at + buf.shape[1]] = jnp.dot(scaled, buf[...], preferred_element_type=F32)
        at += buf.shape[1]
    lane = lax.broadcasted_iota(jnp.int32, (block.shape[0], LANES), 1)
    upper = total.astype(BF16).astype(F32)
    lower = total - upper
    acc[:, at : at + LANES] = jnp.where(lane == 0, upper, jnp.where(lane == 1, lower, 0.0))
    for step, out_ref in enumerate(out_refs):
        out_ref[...] = acc[step * seq_dev : (step + 1) * seq_dev, :].astype(out_ref.dtype)


def split_rows(row):
    upper = row.astype(BF16).astype(F32)
    lower = row - upper
    shape = (8, row.shape[1])
    at = lax.broadcasted_iota(jnp.int32, shape, 0)
    upper = jnp.broadcast_to(upper, shape)
    lower = jnp.broadcast_to(lower, shape)
    return jnp.where(at == 0, upper, jnp.where(at == 1, lower, 0.0)).astype(BF16)


def gather_kernel(
    lengths_ref, _, state_ref, keys_ref, values_ref, rates_ref, gain_ref, mixed_ref, total_ref, own_gain_ref
):
    seq_dev, heads_dev, key_dim, value_dim = state_ref.shape
    span = keys_ref.shape[2]
    row_at = lax.broadcasted_iota(jnp.int32, (span, span), 0)
    col_at = lax.broadcasted_iota(jnp.int32, (span, span), 1)
    upto = jnp.where(col_at <= row_at, 1.0, 0.0).astype(BF16)
    slot = lax.broadcasted_iota(jnp.int32, (span, 1), 0)
    gain = spread(gain_ref)
    columns = own_gain_ref.shape[1]
    member = lax.axis_index("kv") * lax.axis_size("tp") + lax.axis_index("tp")
    own_gain = gain[:, :columns]
    for i in range(1, gain.shape[1] // columns):
        own_gain = jnp.where(member == i, gain[:, i * columns : (i + 1) * columns], own_gain)
    own_gain_ref[...] = own_gain
    for s in range(seq_dev):
        live = (slot < lengths_ref[s]).astype(F32)
        for h in range(heads_dev):
            rates = rates_ref[s, h] * live
            upper = rates.astype(BF16)
            lower = (rates - upper.astype(F32)).astype(BF16)
            running = jnp.dot(upto, upper, preferred_element_type=F32)
            running = running + jnp.dot(upto, lower, preferred_element_type=F32)
            total_ref[s : s + 1, h * key_dim : (h + 1) * key_dim] = running[span - 1 :]
            grown = (jnp.exp(running) * keys_ref[s, h].astype(F32) * live).astype(BF16)
            added = lax.dot_general(
                grown, values_ref[s, h], (((0,), (0,)), ((), ())), preferred_element_type=F32
            )
            mixed_ref[s, h] = (state_ref[s, h] + added).astype(BF16)


def attend_kernel(width, parts, mixed_ref, total_ref, gain_ref, out_ref, heads_ref):
    seq_dev, heads_dev, key_dim, value_dim = mixed_ref.shape
    got = parts[0][...]
    for part in parts[1:]:
        got = got + part[...].astype(F32)
    keys_all, values_all = heads_dev * key_dim, heads_dev * value_dim
    ends = [0, keys_all, 2 * keys_all, 3 * keys_all]
    ends += [ends[3] + values_all, ends[3] + 2 * values_all]
    squares = jnp.sum(got[:, ends[5] :], axis=1, keepdims=True)
    inv_rms = lax.rsqrt(squares / width + EPS)
    query = got[:, ends[0] : ends[1]] * inv_rms * key_dim ** (-0.5)
    key_new = got[:, ends[1] : ends[2]] * inv_rms
    raw = got[:, ends[2] : ends[3]] * inv_rms
    log_decay = (jnp.minimum(raw, 0.0) - jnp.log(1.0 + jnp.exp(-jnp.abs(raw)))) / GATE_NORM
    value_new = got[:, ends[3] : ends[4]] * inv_rms
    gate = got[:, ends[4] : ends[5]] * inv_rms
    gate = gate / (1.0 + jnp.exp(-gate))
    decayed = query * jnp.exp(log_decay - total_ref[...])
    product = query * key_new
    for s in range(seq_dev):
        for h in range(heads_dev):
            ks, vs = slice(h * key_dim, (h + 1) * key_dim), slice(h * value_dim, (h + 1) * value_dim)
            rows = split_rows(decayed[s : s + 1, ks])
            mixed = jnp.dot(rows, mixed_ref[s, h], preferred_element_type=F32)
            own = jnp.sum(product[s : s + 1, ks], axis=1, keepdims=True)
            heads_ref[s : s + 1, vs] = jnp.sum(mixed, axis=0, keepdims=True) + own * value_new[s : s + 1, vs]
    pieces = []
    for h in range(heads_dev):
        vs = slice(h * value_dim, (h + 1) * value_dim)
        attended = heads_ref[:, vs]
        scale = lax.rsqrt(jnp.mean(attended * attended, axis=1, keepdims=True) + EPS)
        pieces.append(gate[:, vs] * (attended * scale * gain_ref[h : h + 1, :].astype(F32)))
    heads = jnp.concatenate(pieces, axis=1).astype(BF16)
    out_ref[...] = heads


def output_kernel(n_kv, *refs):
    near, far = refs[:n_kv], refs[n_kv : 2 * n_kv]
    weight_ref, own_ref, gain_ref, after_ref, scaled_ref = refs[2 * n_kv :]
    half = weight_ref.shape[0] // 2
    tp = lax.axis_index("tp")
    projected = 0.0
    for parts, side in ((near, tp), (far, 1 - tp)):
        rows = jnp.concatenate([part[...].astype(F32) for part in parts], axis=0).astype(BF16)
        weight = weight_ref[pl.ds(pl.multiple_of(side * half, half), half), :]
        projected = projected + jnp.dot(rows, weight, preferred_element_type=F32)
    projected = by_partner(projected, near[0].shape[0], n_kv)
    after = (own_ref[...].astype(F32) + projected).astype(BF16)
    after_ref[...] = after
    after = after.astype(F32)
    columns = after.shape[1]
    scaled_ref[:, :columns] = (after * gain_ref[...]).astype(BF16)
    squares = jnp.sum(after * after, axis=1, keepdims=True)
    lane = lax.broadcasted_iota(jnp.int32, (after.shape[0], LANES), 1)
    upper = squares.astype(BF16).astype(F32)
    lower = squares - upper
    scaled_ref[:, columns:] = jnp.where(lane == 0, upper, jnp.where(lane == 1, lower, 0.0)).astype(BF16)


def member_columns(step, other, columns):
    tp = lax.axis_index("tp")
    tp = 1 - tp if other else tp
    member = (lax.axis_index("kv") ^ step) * lax.axis_size("tp") + tp
    return pl.ds(pl.multiple_of(member * columns, columns), columns)


def grow(cut, columns, pieces, gate_ref, up_ref, tall_refs, flats, squares, fresh):
    contract = (((1,), (1,)), ((), ()))
    for piece, step, other in pieces:
        at = member_columns(step, other, columns)
        rows = piece[:, :columns]
        squares = squares + jnp.sum(piece[:, columns:].astype(F32), axis=1, keepdims=True)
        for j, weight in enumerate((gate_ref, up_ref)):
            tall = lax.dot_general(weight[:cut, at], rows, contract, preferred_element_type=F32)
            tall_refs[j][...] = tall if fresh else tall_refs[j][...] + tall
            flats[j] = flats[j] + lax.dot_general(rows, weight[cut:, at], contract, preferred_element_type=F32)
        fresh = False
    return squares


def first_kernel(cut, columns, own_ref, other_ref, gate_ref, up_ref, _, *sums):
    talls, flat_refs, squares_ref = sums[:2], sums[2:4], sums[4]
    flats = [0.0, 0.0]
    pieces = ((own_ref, 0, False), (other_ref, 0, True))
    squares = grow(cut, columns, pieces, gate_ref, up_ref, talls, flats, 0.0, True)
    for ref, flat in zip(flat_refs, flats):
        ref[...] = flat
    squares_ref[...] = jnp.broadcast_to(squares, squares_ref.shape)


def next_sums(cut, columns, count, other, refs, talls):
    pieces = [(refs[i], i + 1, other) for i in range(count)]
    gate_ref, up_ref = refs[count : count + 2]
    old_talls, flat_refs, squares_ref = refs[count + 2 : count + 4], refs[count + 4 : count + 6], refs[count + 6]
    for new, old in zip(talls, old_talls):
        new[...] = old[...]
    flats = [ref[...] for ref in flat_refs]
    squares = grow(cut, columns, pieces, gate_ref, up_ref, talls, flats, squares_ref[:, :1], False)
    return flats, squares


def second_kernel(cut, columns, count, *refs):
    sums = refs[count + 8 :]
    flats, squares = next_sums(cut, columns, count, False, refs, sums[:2])
    for ref, flat in zip(sums[2:4], flats):
        ref[...] = flat
    sums[4][...] = jnp.broadcast_to(squares, sums[4].shape)


def shares(cut, columns, other, tall, flat, down_ref, out_refs):
    for step, out_ref in enumerate(out_refs):
        at = member_columns(step, other, columns)
        share = lax.dot_general(
            tall, down_ref[:cut, at], (((0,), (0,)), ((), ())), preferred_element_type=F32
        )
        share = share + jnp.dot(flat, down_ref[cut:, at], preferred_element_type=F32)
        out_ref[...] = share.astype(out_ref.dtype)


def third_kernel(cut, columns, count, width, *refs):
    down_ref, (send_ref, tall_ref, flat_ref), talls = refs[count + 7], refs[count + 8 : -2], refs[-2:]
    flats, squares = next_sums(cut, columns, count, True, refs, talls)
    inv = lax.rsqrt(squares / width + EPS)
    rows = inv.shape[0]
    inv_row = jnp.transpose(jnp.broadcast_to(inv, (rows, LANES)))[:1]
    gate = talls[0][...] * inv_row
    tall = (gate / (1.0 + jnp.exp(-gate)) * (talls[1][...] * inv_row)).astype(BF16)
    gate = flats[0] * inv
    flat = (gate / (1.0 + jnp.exp(-gate)) * (flats[1] * inv)).astype(BF16)
    tall_ref[...] = tall
    flat_ref[...] = flat
    outs = [send_ref.at[:, i * columns : (i + 1) * columns] for i in range(count + 1)]
    shares(cut, columns, True, tall, flat, down_ref, outs)


def fourth_kernel(cut, columns, tall_ref, flat_ref, down_ref, out_ref):
    outs = [out_ref.at[:, i * columns : (i + 1) * columns] for i in range(out_ref.shape[1] // columns)]
    shares(cut, columns, False, tall_ref[...], flat_ref[...], down_ref, outs)


def merge_kernel(columns, own_ref, recv_ref, after_ref, *out_refs):
    for step, out_ref in enumerate(out_refs):
        at = slice(step * columns, (step + 1) * columns)
        total = own_ref[:, at] + recv_ref[:, at].astype(F32)
        if step == 0:
            total = total + after_ref[...].astype(F32)
        out_ref[...] = total.astype(out_ref.dtype)


def finish_kernel(*refs):
    total = refs[0][...]
    for part in refs[1:-1]:
        total = total + part[...].astype(F32)
    refs[-1][...] = total.astype(BF16)


MIB = 1 << 20


def shards(
    tokens,
    lengths,
    state,
    cache_keys,
    cache_values,
    cache_rates,
    attn_gain,
    w_query,
    w_key,
    w_value,
    w_gate,
    w_decay,
    head_gain,
    w_out,
    mlp_gain,
    w_mlp_gate,
    w_mlp_up,
    w_mlp_down,
):
    seq_dev, heads_dev, key_dim, value_dim = state.shape
    width = mlp_gain.shape[0]
    n_kv, n_tp = lax.axis_size("kv"), lax.axis_size("tp")
    rows, columns = tokens.shape
    other = lax.ppermute(tokens, "tp", [(i, n_tp - 1 - i) for i in range(n_tp)])
    wide = heads_dev * (3 * key_dim + 2 * value_dim) + LANES
    anywhere = pl.BlockSpec(memory_space=pl.ANY)
    weights = (w_query, w_key, w_decay, w_value, w_gate)
    moved = sum(w.size for w in weights) * 2
    parts = call(
        lambda *refs: project_kernel(seq_dev, *refs),
        [jax.ShapeDtypeStruct((seq_dev, wide), F32 if step == 0 else BF16) for step in range(n_kv)],
        [anywhere, vmem_spec()] + [anywhere] * 6,
        [pltpu.VMEM(tokens.shape, BF16), pltpu.VMEM((attn_gain.size // LANES, LANES), BF16)]
        + [pltpu.VMEM(w.shape, BF16) for w in weights]
        + [pltpu.VMEM((rows, wide), F32), pltpu.SemaphoreType.DMA((7,))],
        16 * MIB,
        10**10,
        moved,
        "project",
    )(in_hbm(tokens), other, in_hbm(attn_gain.reshape(-1, LANES)), *(in_hbm(w) for w in weights))
    parts = list(parts)
    own = parts[0]
    for step in range(1, n_kv):
        parts[step] = lax.ppermute(parts[step], "kv", [(i, i ^ step) for i in range(n_kv)])
    moved = state.size * 6 + cache_rates.size * 8
    mixed, total, own_gain = call(
        gather_kernel,
        [
            jax.ShapeDtypeStruct(state.shape, BF16),
            jax.ShapeDtypeStruct((seq_dev, heads_dev * key_dim), F32),
            jax.ShapeDtypeStruct((1, columns), F32),
        ],
        [pl.BlockSpec(memory_space=pltpu.SMEM), anywhere] + [vmem_spec()] * 5,
        [],
        4 * MIB,
        4 * 10**10,
        moved,
        "gather",
    )(lengths, own, in_vmem(state), in_vmem(cache_keys), in_vmem(cache_values), in_vmem(cache_rates), in_vmem(mlp_gain.reshape(-1, LANES)))
    send = call(
        lambda *refs: attend_kernel(width, refs[:n_kv], *refs[n_kv:]),
        jax.ShapeDtypeStruct((seq_dev, heads_dev * value_dim), BF16),
        [vmem_spec()] * (n_kv + 3),
        [pltpu.VMEM((seq_dev, heads_dev * value_dim), F32)],
        4 * MIB,
        10**6,
        state.size * 2,
        "attend",
    )(own, *parts[:0:-1], mixed, total, in_vmem(head_gain))
    swap = [(i, n_tp - 1 - i) for i in range(n_tp)]
    near = [send] + [
        lax.ppermute(send, "kv", [(i, i ^ step) for i in range(n_kv)]) for step in range(1, n_kv)
    ]
    across = [lax.ppermute(part, "tp", swap) for part in near]
    narrow = jax.ShapeDtypeStruct((rows, columns + LANES), BF16)
    after, scaled = call(
        lambda *refs: output_kernel(n_kv, *refs),
        (jax.ShapeDtypeStruct((rows, columns), BF16), narrow),
        [vmem_spec()] * (2 * n_kv + 3),
        [],
        6 * MIB,
        10**6,
        w_out.size * 2,
        "output",
    )(*near, *across, in_vmem(w_out), in_vmem(tokens), own_gain)
    far = n_kv - 1
    got = [lax.ppermute(scaled, "kv", [(i, i ^ step) for i in range(n_kv)]) for step in range(1, n_kv)]
    beside = lax.ppermute(scaled, "tp", swap)
    hidden = w_mlp_down.shape[0]
    cut = w_mlp_down.shape[0] // 64 * 16
    sums = (
        [jax.ShapeDtypeStruct((cut, rows), F32)] * 2
        + [jax.ShapeDtypeStruct((rows, hidden - cut), F32)] * 2
        + [jax.ShapeDtypeStruct((rows, LANES), F32)]
    )
    down = in_vmem(w_mlp_down)
    gate_up = (in_vmem(w_mlp_gate.T), in_vmem(w_mlp_up.T))
    running = call(
        lambda *refs: first_kernel(cut, columns, *refs),
        sums,
        [vmem_spec()] * 5,
        [],
        4 * MIB,
        MIB,
        MIB,
        "feed_first",
    )(scaled, beside, *gate_up, down)
    got, running = lax.optimization_barrier((got, running))
    beside = [lax.ppermute(piece, "tp", swap) for piece in got]
    running = call(
        lambda *refs: second_kernel(cut, columns, far, *refs),
        sums,
        [vmem_spec()] * (far + 8),
        [],
        4 * MIB,
        MIB,
        MIB,
        "feed_second",
    )(*got, *gate_up, *running, down)
    send, tall, flat = call(
        lambda *refs: third_kernel(cut, columns, far, width, *refs),
        [
            jax.ShapeDtypeStruct((rows, n_kv * columns), BF16),
            jax.ShapeDtypeStruct((cut, rows), BF16),
            jax.ShapeDtypeStruct((rows, hidden - cut), BF16),
        ],
        [vmem_spec()] * (far + 8),
        [pltpu.VMEM((cut, rows), F32)] * 2,
        4 * MIB,
        MIB,
        MIB,
        "feed_third",
    )(*beside, *gate_up, *running, down)
    recv = lax.ppermute(send, "tp", swap)
    own = call(
        lambda *refs: fourth_kernel(cut, columns, *refs),
        jax.ShapeDtypeStruct((rows, n_kv * columns), F32),
        [vmem_spec()] * 3,
        [],
        4 * MIB,
        MIB,
        MIB,
        "feed_fourth",
    )(tall, flat, down)
    merged = call(
        lambda *refs: merge_kernel(columns, *refs),
        [jax.ShapeDtypeStruct((rows, columns), F32 if step == 0 else BF16) for step in range(n_kv)],
        [vmem_spec()] * 3,
        [],
        2 * MIB,
        rows * columns * n_kv,
        rows * columns * n_kv * 6,
        "merge",
    )(own, recv, after)
    parts = [
        lax.ppermute(merged[step], "kv", [(i, i ^ step) for i in range(n_kv)]) for step in range(1, n_kv)
    ]
    return call(
        finish_kernel,
        jax.ShapeDtypeStruct((rows, columns), BF16),
        [vmem_spec()] * n_kv,
        [],
        2 * MIB,
        rows * columns * n_kv,
        rows * columns * n_kv * 2,
        "finish",
    )(merged[0], *parts[::-1])


def solution(mesh):
    placed = (
        P("dp", ("kv", "tp")),
        P(("dp", "kv")),
        P(("dp", "kv"), "tp", None, None),
        P(("dp", "kv"), "tp", None, None),
        P(("dp", "kv"), "tp", None, None),
        P(("dp", "kv"), "tp", None, None),
        P("kv"),
        P("kv", "tp"),
        P("kv", "tp"),
        P("kv", "tp"),
        P("kv", "tp"),
        P("kv", "tp"),
        P("tp", None),
        P(None, ("kv", "tp")),
        P(),
        P(None, ("kv", "tp")),
        P(None, ("kv", "tp")),
        P(("kv", "tp"), None),
    )
    sizes = mesh.shape

    def body(*args):
        fits = sizes["tp"] == 2 and sizes["kv"] == 4 and args[13].shape[1] % LANES == 0
        return (shards if fits else plain_shards)(*args)

    return jax.shard_map(
        body, mesh=mesh, in_specs=placed, out_specs=P("dp", ("kv", "tp")), check_vma=False
    )
```

```python
import jax
import jax.numpy as jnp
from jax import lax
from jax.experimental import pallas as pl
from jax.experimental.pallas import tpu as pltpu
from jax.sharding import PartitionSpec as P

EPS = 1e-06
GATE_NORM = 16.0
exact_mode = lax.Precision.HIGHEST


def front_part(query, key_new, log_decay, state, cache_keys, cache_rates, lengths):
    span = cache_keys.shape[2]
    live = (jnp.arange(span, dtype=jnp.int32)[None, :] < lengths[:, None]).astype(jnp.float32)
    running = jnp.cumsum(cache_rates * live[:, None, :, None], axis=2)
    total = running[:, :, -1:, :]
    weight = jnp.exp(running - total + log_decay[:, :, None, :])
    scores = (
        jnp.einsum(
            "bhd,bhjd->bhj", query, weight * cache_keys.astype(jnp.float32), precision=exact_mode
        )
        * live[:, None, :]
    )
    carried = jnp.einsum(
        "bhd,bhde->bhe", query * jnp.exp(log_decay - total[:, :, 0, :]), state, precision=exact_mode
    )
    own = jnp.sum(query * key_new, axis=-1, keepdims=True)
    return (scores, carried, own)


def back_part(scores, carried, own, value_new, cache_values, gate, head_gain):
    inner = jnp.einsum(
        "bhj,bhje->bhe", scores, cache_values.astype(jnp.float32), precision=exact_mode
    )
    attended = carried + inner + own * value_new
    normed = attended * lax.rsqrt(jnp.mean(attended * attended, axis=-1, keepdims=True) + EPS)
    normed = normed * head_gain.astype(jnp.float32)
    return (jax.nn.silu(gate) * normed).astype(jnp.bfloat16)


def open_heads(
    query_sum, key_sum, decay_sum, own_squares, width, state, cache_keys, cache_rates, lengths
):
    seq_dev, heads_dev, key_dim = (state.shape[0], state.shape[1], state.shape[2])
    inv_rms = lax.rsqrt(own_squares / width + EPS)[:, None]
    query = (query_sum * inv_rms * key_dim ** (-0.5)).reshape(seq_dev, heads_dev, key_dim)
    key_new = (key_sum * inv_rms).reshape(seq_dev, heads_dev, key_dim)
    log_decay = (jax.nn.log_sigmoid(decay_sum * inv_rms) / GATE_NORM).reshape(
        seq_dev, heads_dev, key_dim
    )
    scores, carried, own = front_part(
        query, key_new, log_decay, state, cache_keys, cache_rates, lengths
    )
    return (inv_rms, scores, carried, own)


def close_heads(opened, value_sum, gate_sum, cache_values, head_gain):
    inv_rms, scores, carried, own = opened
    seq_dev, heads_dev, value_dim = carried.shape
    value_new = (value_sum * inv_rms).reshape(seq_dev, heads_dev, value_dim)
    gate = (gate_sum * inv_rms).reshape(seq_dev, heads_dev, value_dim)
    heads = back_part(scores, carried, own, value_new, cache_values, gate, head_gain)
    return heads.reshape(seq_dev, heads_dev * value_dim)


def plain_shards(
    tokens,
    lengths,
    state,
    cache_keys,
    cache_values,
    cache_rates,
    attn_gain,
    w_query,
    w_key,
    w_value,
    w_gate,
    w_decay,
    head_gain,
    w_out,
    mlp_gain,
    w_mlp_gate,
    w_mlp_up,
    w_mlp_down,
):
    seq_dev, heads_dev, value_dim = (state.shape[0], state.shape[1], state.shape[3])
    width = mlp_gain.shape[0]
    n_kv = lax.axis_size("kv")
    n_tp = lax.axis_size("tp")
    block = lax.all_gather(tokens, "tp", axis=1, tiled=True).astype(jnp.float32)
    squares = jnp.sum(block * block, axis=1)
    scaled = (block * attn_gain.astype(jnp.float32)).astype(jnp.bfloat16)
    query_part = jnp.dot(scaled, w_query, preferred_element_type=jnp.float32)
    key_part = jnp.dot(scaled, w_key, preferred_element_type=jnp.float32)
    decay_part = jnp.dot(scaled, w_decay, preferred_element_type=jnp.float32)
    value_part = jnp.dot(scaled, w_value, preferred_element_type=jnp.float32)
    gate_part = jnp.dot(scaled, w_gate, preferred_element_type=jnp.float32)
    every_square = lax.psum(squares, "kv")
    own_squares = lax.dynamic_slice_in_dim(every_square, lax.axis_index("kv") * seq_dev, seq_dev)
    query_sum, key_sum, decay_sum, value_sum, gate_sum = (
        lax.psum_scatter(query_part, "kv", scatter_dimension=0, tiled=True),
        lax.psum_scatter(key_part, "kv", scatter_dimension=0, tiled=True),
        lax.psum_scatter(decay_part, "kv", scatter_dimension=0, tiled=True),
        lax.psum_scatter(value_part, "kv", scatter_dimension=0, tiled=True),
        lax.psum_scatter(gate_part, "kv", scatter_dimension=0, tiled=True),
    )
    opened = open_heads(
        query_sum, key_sum, decay_sum, own_squares, width, state, cache_keys, cache_rates, lengths
    )
    heads = close_heads(opened, value_sum, gate_sum, cache_values, head_gain)
    columns = w_out.shape[1]
    stacked = w_out.reshape(n_tp, heads_dev * value_dim, columns)
    piece = lax.all_gather(
        heads.reshape(1, seq_dev, heads_dev * value_dim), ("kv", "tp"), axis=0, tiled=True
    )
    terms = jnp.einsum("psk,tkc->ptsc", piece, stacked, preferred_element_type=jnp.float32)
    owner = jnp.arange(piece.shape[0], dtype=jnp.int32)
    row_match = (owner // n_tp)[:, None, None] == jnp.arange(n_kv, dtype=jnp.int32)[None, :, None]
    head_match = (owner % n_tp)[:, None, None] == jnp.arange(n_tp, dtype=jnp.int32)[None, None, :]
    chosen = (row_match & head_match).astype(jnp.float32)
    projected = jnp.einsum("prt,ptsc->rsc", chosen, terms, precision=exact_mode)
    projected = projected.reshape(n_kv * seq_dev, columns)
    after = (tokens.astype(jnp.float32) + projected).astype(jnp.bfloat16)
    whole = lax.all_gather(after, ("kv", "tp"), axis=1, tiled=True).astype(jnp.float32)
    inv_second = lax.rsqrt(jnp.mean(whole * whole, axis=1, keepdims=True) + EPS)
    normed = (whole * inv_second * mlp_gain.astype(jnp.float32)).astype(jnp.bfloat16)
    gate_ff = jnp.dot(normed, w_mlp_gate, preferred_element_type=jnp.float32)
    up_ff = jnp.dot(normed, w_mlp_up, preferred_element_type=jnp.float32)
    hidden = (jax.nn.silu(gate_ff) * up_ff).astype(jnp.bfloat16)
    terms = jnp.dot(hidden, w_mlp_down, preferred_element_type=jnp.float32)
    own_share = lax.psum_scatter(terms, ("kv", "tp"), scatter_dimension=1, tiled=True)
    return (after.astype(jnp.float32) + own_share).astype(jnp.bfloat16)


F32 = jnp.float32
BF16 = jnp.bfloat16
LANES = 128


def in_vmem(array):
    return pltpu.with_memory_space_constraint(array, pltpu.VMEM)


def in_hbm(array):
    return pltpu.with_memory_space_constraint(array, pltpu.HBM)


def vmem_spec():
    return pl.BlockSpec(memory_space=pltpu.VMEM)


def call(kernel, out_shape, in_specs, scratch, limit, flops, moved, name):
    return pl.pallas_call(
        kernel,
        out_shape=out_shape,
        in_specs=in_specs,
        out_specs=jax.tree.map(lambda _: vmem_spec(), out_shape),
        scratch_shapes=scratch,
        compiler_params=pltpu.CompilerParams(vmem_limit_bytes=limit),
        cost_estimate=pl.CostEstimate(flops=flops, bytes_accessed=moved, transcendentals=0),
        name=name,
    )


def spread(gain_ref):
    rows = gain_ref[...].astype(F32)
    return jnp.concatenate([rows[i : i + 1] for i in range(rows.shape[0])], axis=1)


def by_partner(block, seq_dev, n_kv):
    me = lax.axis_index("kv")
    place = lax.broadcasted_iota(jnp.int32, block.shape, 0) // seq_dev
    rows = block.shape[0]
    bit = 1
    while bit < n_kv:
        down = pltpu.roll(block, bit * seq_dev, 0)
        up = pltpu.roll(block, rows - bit * seq_dev, 0)
        swapped = jnp.where((place & bit) == 0, up, down)
        block = jnp.where((me & bit) == 0, block, swapped)
        bit *= 2
    return block


def scale_half(half, gain, seq_dev, n_kv):
    ordered = by_partner(half.astype(F32), seq_dev, n_kv)
    squares = jnp.sum(ordered * ordered, axis=1, keepdims=True)
    return (ordered * gain).astype(BF16), jnp.broadcast_to(squares, (half.shape[0], LANES))


def half_gain(gain_ref, own):
    gain = spread(gain_ref)
    half = gain.shape[1] // 2
    low = (lax.axis_index("tp") == 0) == own
    return jnp.where(low, gain[:, :half], gain[:, half:])


def prepare_kernel(seq_dev, n_kv, own_hbm, gain_hbm, scaled_ref, squares_ref, own_ref, gain_ref, sems):
    copies = [
        pltpu.make_async_copy(own_hbm, own_ref, sems.at[0]),
        pltpu.make_async_copy(gain_hbm, gain_ref, sems.at[1]),
    ]
    for copy in copies:
        copy.start()
    for copy in copies:
        copy.wait()
    scaled_ref[...], squares_ref[...] = scale_half(own_ref[...], half_gain(gain_ref, True), seq_dev, n_kv)


def values_kernel(seq_dev, n_kv, scaled_ref, squares_ref, other_ref, gain_ref, wv, wg, sums_ref, block_ref, total_ref):
    scaled, squares = scale_half(other_ref[...], half_gain(gain_ref, False), seq_dev, n_kv)
    total_ref[...] = squares_ref[...] + squares
    own = scaled_ref[...].astype(F32)
    scaled = scaled.astype(F32)
    first = lax.axis_index("tp") == 0
    block = jnp.concatenate([jnp.where(first, own, scaled), jnp.where(first, scaled, own)], axis=1).astype(BF16)
    block_ref[...] = block
    cut = wv.shape[1]
    sums_ref[:, :cut] = jnp.dot(block, wv[...], preferred_element_type=F32)
    sums_ref[:, cut:] = jnp.dot(block, wg[...], preferred_element_type=F32)


def keys_kernel(seq_dev, block_ref, total_ref, sums_ref, wq, wk, wd, *rest):
    out_refs, acc = rest[:-1], rest[-1]
    block = block_ref[...]
    at = 0
    for weight in (wq, wk, wd):
        acc[:, at : at + weight.shape[1]] = jnp.dot(block, weight[...], preferred_element_type=F32)
        at += weight.shape[1]
    total = total_ref[...]
    lane = lax.broadcasted_iota(jnp.int32, total.shape, 1)
    upper = total.astype(BF16).astype(F32)
    lower = total - upper
    squares = jnp.where(lane == 0, upper, jnp.where(lane == 1, lower, 0.0))
    for step, out_ref in enumerate(out_refs):
        take = slice(step * seq_dev, (step + 1) * seq_dev)
        out_ref[:, :at] = acc[take, :].astype(out_ref.dtype)
        out_ref[:, at : at + sums_ref.shape[1]] = sums_ref[take, :].astype(out_ref.dtype)
        out_ref[:, at + sums_ref.shape[1] :] = squares[take, :].astype(out_ref.dtype)


def split_rows(row):
    upper = row.astype(BF16).astype(F32)
    lower = row - upper
    shape = (8, row.shape[1])
    at = lax.broadcasted_iota(jnp.int32, shape, 0)
    upper = jnp.broadcast_to(upper, shape)
    lower = jnp.broadcast_to(lower, shape)
    return jnp.where(at == 0, upper, jnp.where(at == 1, lower, 0.0)).astype(BF16)


def gather_kernel(
    lengths_ref, _, state_ref, keys_ref, values_ref, rates_ref, gain_ref, mixed_ref, total_ref, own_gain_ref
):
    seq_dev, heads_dev, key_dim, value_dim = state_ref.shape
    span = keys_ref.shape[2]
    row_at = lax.broadcasted_iota(jnp.int32, (span, span), 0)
    col_at = lax.broadcasted_iota(jnp.int32, (span, span), 1)
    upto = jnp.where(col_at <= row_at, 1.0, 0.0).astype(BF16)
    slot = lax.broadcasted_iota(jnp.int32, (span, 1), 0)
    gain = spread(gain_ref)
    columns = own_gain_ref.shape[1]
    member = lax.axis_index("kv") * lax.axis_size("tp") + lax.axis_index("tp")
    own_gain = gain[:, :columns]
    for i in range(1, gain.shape[1] // columns):
        own_gain = jnp.where(member == i, gain[:, i * columns : (i + 1) * columns], own_gain)
    own_gain_ref[...] = own_gain
    for s in range(seq_dev):
        live = (slot < lengths_ref[s]).astype(F32)
        for h in range(heads_dev):
            rates = rates_ref[s, h] * live
            upper = rates.astype(BF16)
            lower = (rates - upper.astype(F32)).astype(BF16)
            running = jnp.dot(upto, upper, preferred_element_type=F32)
            running = running + jnp.dot(upto, lower, preferred_element_type=F32)
            total_ref[s : s + 1, h * key_dim : (h + 1) * key_dim] = running[span - 1 :]
            grown = (jnp.exp(running) * keys_ref[s, h].astype(F32) * live).astype(BF16)
            added = lax.dot_general(
                grown, values_ref[s, h], (((0,), (0,)), ((), ())), preferred_element_type=F32
            )
            mixed_ref[s, h] = (state_ref[s, h] + added).astype(BF16)


def attend_kernel(width, parts, mixed_ref, total_ref, gain_ref, out_ref, heads_ref):
    seq_dev, heads_dev, key_dim, value_dim = mixed_ref.shape
    got = parts[0][...]
    for part in parts[1:]:
        got = got + part[...].astype(F32)
    keys_all, values_all = heads_dev * key_dim, heads_dev * value_dim
    ends = [0, keys_all, 2 * keys_all, 3 * keys_all]
    ends += [ends[3] + values_all, ends[3] + 2 * values_all]
    squares = jnp.sum(got[:, ends[5] :], axis=1, keepdims=True)
    inv_rms = lax.rsqrt(squares / width + EPS)
    query = got[:, ends[0] : ends[1]] * inv_rms * key_dim ** (-0.5)
    key_new = got[:, ends[1] : ends[2]] * inv_rms
    raw = got[:, ends[2] : ends[3]] * inv_rms
    log_decay = (jnp.minimum(raw, 0.0) - jnp.log(1.0 + jnp.exp(-jnp.abs(raw)))) / GATE_NORM
    value_new = got[:, ends[3] : ends[4]] * inv_rms
    gate = got[:, ends[4] : ends[5]] * inv_rms
    gate = gate / (1.0 + jnp.exp(-gate))
    decayed = query * jnp.exp(log_decay - total_ref[...])
    product = query * key_new
    for s in range(seq_dev):
        for h in range(heads_dev):
            ks, vs = slice(h * key_dim, (h + 1) * key_dim), slice(h * value_dim, (h + 1) * value_dim)
            rows = split_rows(decayed[s : s + 1, ks])
            mixed = jnp.dot(rows, mixed_ref[s, h], preferred_element_type=F32)
            own = jnp.sum(product[s : s + 1, ks], axis=1, keepdims=True)
            heads_ref[s : s + 1, vs] = jnp.sum(mixed, axis=0, keepdims=True) + own * value_new[s : s + 1, vs]
    pieces = []
    for h in range(heads_dev):
        vs = slice(h * value_dim, (h + 1) * value_dim)
        attended = heads_ref[:, vs]
        scale = lax.rsqrt(jnp.mean(attended * attended, axis=1, keepdims=True) + EPS)
        pieces.append(gate[:, vs] * (attended * scale * gain_ref[h : h + 1, :].astype(F32)))
    heads = jnp.concatenate(pieces, axis=1).astype(BF16)
    out_ref[...] = heads


def output_kernel(n_kv, *refs):
    near, far = refs[:n_kv], refs[n_kv : 2 * n_kv]
    weight_ref, own_ref, gain_ref, after_ref, scaled_ref = refs[2 * n_kv :]
    half = weight_ref.shape[0] // 2
    tp = lax.axis_index("tp")
    projected = 0.0
    for parts, side in ((near, tp), (far, 1 - tp)):
        rows = jnp.concatenate([part[...].astype(F32) for part in parts], axis=0).astype(BF16)
        weight = weight_ref[pl.ds(pl.multiple_of(side * half, half), half), :]
        projected = projected + jnp.dot(rows, weight, preferred_element_type=F32)
    projected = by_partner(projected, near[0].shape[0], n_kv)
    after = (own_ref[...].astype(F32) + projected).astype(BF16)
    after_ref[...] = after
    after = after.astype(F32)
    columns = after.shape[1]
    scaled_ref[:, :columns] = (after * gain_ref[...]).astype(BF16)
    squares = jnp.sum(after * after, axis=1, keepdims=True)
    lane = lax.broadcasted_iota(jnp.int32, (after.shape[0], LANES), 1)
    upper = squares.astype(BF16).astype(F32)
    lower = squares - upper
    scaled_ref[:, columns:] = jnp.where(lane == 0, upper, jnp.where(lane == 1, lower, 0.0)).astype(BF16)


def member_columns(step, other, columns):
    tp = lax.axis_index("tp")
    tp = 1 - tp if other else tp
    member = (lax.axis_index("kv") ^ step) * lax.axis_size("tp") + tp
    return pl.ds(pl.multiple_of(member * columns, columns), columns)


def grow(cut, columns, pieces, gate_ref, up_ref, tall_refs, flats, squares, fresh):
    contract = (((1,), (1,)), ((), ()))
    for piece, step, other in pieces:
        at = member_columns(step, other, columns)
        rows = piece[:, :columns]
        squares = squares + jnp.sum(piece[:, columns:].astype(F32), axis=1, keepdims=True)
        for j, weight in enumerate((gate_ref, up_ref)):
            tall = lax.dot_general(weight[:cut, at], rows, contract, preferred_element_type=F32)
            tall_refs[j][...] = tall if fresh else tall_refs[j][...] + tall
            flats[j] = flats[j] + lax.dot_general(rows, weight[cut:, at], contract, preferred_element_type=F32)
        fresh = False
    return squares


def first_kernel(cut, columns, own_ref, other_ref, gate_ref, up_ref, _, *sums):
    talls, flat_refs, squares_ref = sums[:2], sums[2:4], sums[4]
    flats = [0.0, 0.0]
    pieces = ((own_ref, 0, False), (other_ref, 0, True))
    squares = grow(cut, columns, pieces, gate_ref, up_ref, talls, flats, 0.0, True)
    for ref, flat in zip(flat_refs, flats):
        ref[...] = flat
    squares_ref[...] = jnp.broadcast_to(squares, squares_ref.shape)


def next_sums(cut, columns, count, other, refs, talls):
    pieces = [(refs[i], i + 1, other) for i in range(count)]
    gate_ref, up_ref = refs[count : count + 2]
    old_talls, flat_refs, squares_ref = refs[count + 2 : count + 4], refs[count + 4 : count + 6], refs[count + 6]
    for new, old in zip(talls, old_talls):
        new[...] = old[...]
    flats = [ref[...] for ref in flat_refs]
    squares = grow(cut, columns, pieces, gate_ref, up_ref, talls, flats, squares_ref[:, :1], False)
    return flats, squares


def second_kernel(cut, columns, count, *refs):
    sums = refs[count + 8 :]
    flats, squares = next_sums(cut, columns, count, False, refs, sums[:2])
    for ref, flat in zip(sums[2:4], flats):
        ref[...] = flat
    sums[4][...] = jnp.broadcast_to(squares, sums[4].shape)


def shares(cut, columns, other, tall, flat, down_ref, out_refs):
    for step, out_ref in enumerate(out_refs):
        at = member_columns(step, other, columns)
        share = lax.dot_general(
            tall, down_ref[:cut, at], (((0,), (0,)), ((), ())), preferred_element_type=F32
        )
        share = share + jnp.dot(flat, down_ref[cut:, at], preferred_element_type=F32)
        out_ref[...] = share.astype(out_ref.dtype)


def third_kernel(cut, columns, count, width, *refs):
    down_ref, (send_ref, tall_ref, flat_ref), talls = refs[count + 7], refs[count + 8 : -2], refs[-2:]
    flats, squares = next_sums(cut, columns, count, True, refs, talls)
    inv = lax.rsqrt(squares / width + EPS)
    rows = inv.shape[0]
    inv_row = jnp.transpose(jnp.broadcast_to(inv, (rows, LANES)))[:1]
    gate = talls[0][...] * inv_row
    tall = (gate / (1.0 + jnp.exp(-gate)) * (talls[1][...] * inv_row)).astype(BF16)
    gate = flats[0] * inv
    flat = (gate / (1.0 + jnp.exp(-gate)) * (flats[1] * inv)).astype(BF16)
    tall_ref[...] = tall
    flat_ref[...] = flat
    outs = [send_ref.at[:, i * columns : (i + 1) * columns] for i in range(count + 1)]
    shares(cut, columns, True, tall, flat, down_ref, outs)


def fourth_kernel(cut, columns, tall_ref, flat_ref, down_ref, out_ref):
    outs = [out_ref.at[:, i * columns : (i + 1) * columns] for i in range(out_ref.shape[1] // columns)]
    shares(cut, columns, False, tall_ref[...], flat_ref[...], down_ref, outs)


def merge_kernel(columns, own_ref, recv_ref, after_ref, *out_refs):
    for step, out_ref in enumerate(out_refs):
        at = slice(step * columns, (step + 1) * columns)
        total = own_ref[:, at] + recv_ref[:, at].astype(F32)
        if step == 0:
            total = total + after_ref[...].astype(F32)
        out_ref[...] = total.astype(out_ref.dtype)


def finish_kernel(*refs):
    total = refs[0][...]
    for part in refs[1:-1]:
        total = total + part[...].astype(F32)
    refs[-1][...] = total.astype(BF16)


MIB = 1 << 20


def shards(
    tokens,
    lengths,
    state,
    cache_keys,
    cache_values,
    cache_rates,
    attn_gain,
    w_query,
    w_key,
    w_value,
    w_gate,
    w_decay,
    head_gain,
    w_out,
    mlp_gain,
    w_mlp_gate,
    w_mlp_up,
    w_mlp_down,
):
    seq_dev, heads_dev, key_dim, value_dim = state.shape
    width = mlp_gain.shape[0]
    n_kv, n_tp = lax.axis_size("kv"), lax.axis_size("tp")
    rows, columns = tokens.shape
    other = lax.ppermute(tokens, "tp", [(i, n_tp - 1 - i) for i in range(n_tp)])
    wide = heads_dev * (3 * key_dim + 2 * value_dim) + LANES
    anywhere = pl.BlockSpec(memory_space=pl.ANY)
    gain_rows = attn_gain.reshape(-1, LANES)
    scaled, squares = call(
        lambda *refs: prepare_kernel(seq_dev, n_kv, *refs),
        [jax.ShapeDtypeStruct(tokens.shape, BF16), jax.ShapeDtypeStruct((rows, LANES), F32)],
        [anywhere] * 2,
        [
            pltpu.VMEM(tokens.shape, BF16),
            pltpu.VMEM(gain_rows.shape, BF16),
            pltpu.SemaphoreType.DMA((2,)),
        ],
        MIB,
        10**10,
        tokens.size * 2,
        "prepare",
    )(in_hbm(tokens), in_hbm(gain_rows))
    late = 2 * heads_dev * value_dim
    sums, block, squares = call(
        lambda *refs: values_kernel(seq_dev, n_kv, *refs),
        [
            jax.ShapeDtypeStruct((rows, late), F32),
            jax.ShapeDtypeStruct((rows, n_tp * columns), BF16),
            jax.ShapeDtypeStruct((rows, LANES), F32),
        ],
        [vmem_spec()] * 6,
        [],
        4 * MIB,
        10**6,
        MIB,
        "values",
    )(scaled, squares, other, in_vmem(gain_rows), in_vmem(w_value), in_vmem(w_gate))
    parts = call(
        lambda *refs: keys_kernel(seq_dev, *refs),
        [jax.ShapeDtypeStruct((seq_dev, wide), F32 if step == 0 else BF16) for step in range(n_kv)],
        [vmem_spec()] * 6,
        [pltpu.VMEM((rows, wide - LANES - late), F32)],
        4 * MIB,
        10**10,
        MIB,
        "keys",
    )(block, squares, sums, in_vmem(w_query), in_vmem(w_key), in_vmem(w_decay))
    parts = list(parts)
    own = parts[0]
    for step in range(1, n_kv):
        parts[step] = lax.ppermute(parts[step], "kv", [(i, i ^ step) for i in range(n_kv)])
    moved = state.size * 6 + cache_rates.size * 8
    mixed, total, own_gain = call(
        gather_kernel,
        [
            jax.ShapeDtypeStruct(state.shape, BF16),
            jax.ShapeDtypeStruct((seq_dev, heads_dev * key_dim), F32),
            jax.ShapeDtypeStruct((1, columns), F32),
        ],
        [pl.BlockSpec(memory_space=pltpu.SMEM), anywhere] + [vmem_spec()] * 5,
        [],
        4 * MIB,
        4 * 10**10,
        moved,
        "gather",
    )(lengths, own, in_vmem(state), in_vmem(cache_keys), in_vmem(cache_values), in_vmem(cache_rates), in_vmem(mlp_gain.reshape(-1, LANES)))
    send = call(
        lambda *refs: attend_kernel(width, refs[:n_kv], *refs[n_kv:]),
        jax.ShapeDtypeStruct((seq_dev, heads_dev * value_dim), BF16),
        [vmem_spec()] * (n_kv + 3),
        [pltpu.VMEM((seq_dev, heads_dev * value_dim), F32)],
        4 * MIB,
        10**6,
        state.size * 2,
        "attend",
    )(own, *parts[:0:-1], mixed, total, in_vmem(head_gain))
    swap = [(i, n_tp - 1 - i) for i in range(n_tp)]
    near = [send] + [
        lax.ppermute(send, "kv", [(i, i ^ step) for i in range(n_kv)]) for step in range(1, n_kv)
    ]
    across = [lax.ppermute(part, "tp", swap) for part in near]
    narrow = jax.ShapeDtypeStruct((rows, columns + LANES), BF16)
    after, scaled = call(
        lambda *refs: output_kernel(n_kv, *refs),
        (jax.ShapeDtypeStruct((rows, columns), BF16), narrow),
        [vmem_spec()] * (2 * n_kv + 3),
        [],
        6 * MIB,
        10**6,
        w_out.size * 2,
        "output",
    )(*near, *across, in_vmem(w_out), in_vmem(tokens), own_gain)
    far = n_kv - 1
    got = [lax.ppermute(scaled, "kv", [(i, i ^ step) for i in range(n_kv)]) for step in range(1, n_kv)]
    beside = lax.ppermute(scaled, "tp", swap)
    hidden = w_mlp_down.shape[0]
    cut = w_mlp_down.shape[0] // 64 * 16
    sums = (
        [jax.ShapeDtypeStruct((cut, rows), F32)] * 2
        + [jax.ShapeDtypeStruct((rows, hidden - cut), F32)] * 2
        + [jax.ShapeDtypeStruct((rows, LANES), F32)]
    )
    down = in_vmem(w_mlp_down)
    gate_up = (in_vmem(w_mlp_gate.T), in_vmem(w_mlp_up.T))
    running = call(
        lambda *refs: first_kernel(cut, columns, *refs),
        sums,
        [vmem_spec()] * 5,
        [],
        4 * MIB,
        MIB,
        MIB,
        "feed_first",
    )(scaled, beside, *gate_up, down)
    got, running = lax.optimization_barrier((got, running))
    beside = [lax.ppermute(piece, "tp", swap) for piece in got]
    running = call(
        lambda *refs: second_kernel(cut, columns, far, *refs),
        sums,
        [vmem_spec()] * (far + 8),
        [],
        4 * MIB,
        MIB,
        MIB,
        "feed_second",
    )(*got, *gate_up, *running, down)
    send, tall, flat = call(
        lambda *refs: third_kernel(cut, columns, far, width, *refs),
        [
            jax.ShapeDtypeStruct((rows, n_kv * columns), BF16),
            jax.ShapeDtypeStruct((cut, rows), BF16),
            jax.ShapeDtypeStruct((rows, hidden - cut), BF16),
        ],
        [vmem_spec()] * (far + 8),
        [pltpu.VMEM((cut, rows), F32)] * 2,
        4 * MIB,
        MIB,
        MIB,
        "feed_third",
    )(*beside, *gate_up, *running, down)
    recv = lax.ppermute(send, "tp", swap)
    own = call(
        lambda *refs: fourth_kernel(cut, columns, *refs),
        jax.ShapeDtypeStruct((rows, n_kv * columns), F32),
        [vmem_spec()] * 3,
        [],
        4 * MIB,
        MIB,
        MIB,
        "feed_fourth",
    )(tall, flat, down)
    merged = call(
        lambda *refs: merge_kernel(columns, *refs),
        [jax.ShapeDtypeStruct((rows, columns), F32 if step == 0 else BF16) for step in range(n_kv)],
        [vmem_spec()] * 3,
        [],
        2 * MIB,
        rows * columns * n_kv,
        rows * columns * n_kv * 6,
        "merge",
    )(own, recv, after)
    parts = [
        lax.ppermute(merged[step], "kv", [(i, i ^ step) for i in range(n_kv)]) for step in range(1, n_kv)
    ]
    return call(
        finish_kernel,
        jax.ShapeDtypeStruct((rows, columns), BF16),
        [vmem_spec()] * n_kv,
        [],
        2 * MIB,
        rows * columns * n_kv,
        rows * columns * n_kv * 2,
        "finish",
    )(merged[0], *parts[::-1])


def solution(mesh):
    placed = (
        P("dp", ("kv", "tp")),
        P(("dp", "kv")),
        P(("dp", "kv"), "tp", None, None),
        P(("dp", "kv"), "tp", None, None),
        P(("dp", "kv"), "tp", None, None),
        P(("dp", "kv"), "tp", None, None),
        P("kv"),
        P("kv", "tp"),
        P("kv", "tp"),
        P("kv", "tp"),
        P("kv", "tp"),
        P("kv", "tp"),
        P("tp", None),
        P(None, ("kv", "tp")),
        P(),
        P(None, ("kv", "tp")),
        P(None, ("kv", "tp")),
        P(("kv", "tp"), None),
    )
    sizes = mesh.shape

    def body(*args):
        fits = sizes["tp"] == 2 and sizes["kv"] == 4 and args[13].shape[1] % LANES == 0
        return (shards if fits else plain_shards)(*args)

    return jax.shard_map(
        body, mesh=mesh, in_specs=placed, out_specs=P("dp", ("kv", "tp")), check_vma=False
    )
```
